256 devices in a mesh: sp: 16 (over y, x), tp: 16 (over z, core).
Axes of the slice: x: 4, y: 4, z: 8, core: 2. Of those that a mesh axis runs over, the one named last changes fastest.
Arguments:
- residual_in: bfloat16 [8192, 4096], P('sp', 'tp'), may hold values from -24 to 24
- norm_gain: float32 [2, 4096], replicated, may hold values from 0.1 to 1.9
- gate_proj: bfloat16 [2, 4096, 2048], P(None, 'sp', 'tp'), may hold values from -0.09375 to 0.09375
- filter_proj: bfloat16 [2, 4096, 2048], P(None, 'sp', 'tp'), may hold values from -0.09375 to 0.09375
- signal_proj: bfloat16 [2, 4096, 2048], P(None, 'sp', 'tp'), may hold values from -0.09375 to 0.09375
- conv_taps: float32 [2, 3, 2048], P(None, None, 'tp'), may hold values from -3 to 3
- out_proj: bfloat16 [2, 2048, 4096], P(None, 'tp', 'sp'), may hold values from -0.1875 to 0.1875
- final_gain: float32 [4096], P('tp'), may hold values from 0.1 to 1.9
Outputs:
- final_rows: float32 [8192, 4096], P('sp', 'tp')
The draws below stay inside these ranges and needn't reach their ends.
All inputs are finite; a program needn't handle non-finite values.
Results may differ from the reference program's by a relative error of at most 0.033.
Values may be sent and summed in bfloat16 or wider, within the bound.
A program may use at most 64 MiB of HBM per device.

```python
import math
import jax
import jax.numpy as jnp
from jax import lax

D = 4096
CW = 2048
TAPS = 3
LAYERS = 2
TOKENS = 8192
N_TP = 16


def draw_residual_in(key, part):
    subkeys = jax.random.split(key, 4)
    standard = jax.random.normal(subkeys[0], (TOKENS, D), jnp.float32)
    group_scale = jnp.exp(jax.random.uniform(subkeys[1], (D // 64,), jnp.float32, math.log(0.3), math.log(3.0)))
    column_scale = jnp.repeat(group_scale, 64)
    values = standard * column_scale[None, :]
    return jnp.clip(values, -24.0, 24.0).astype(jnp.bfloat16)


def spiked(values, rng, source, target, shards_of, factor):
    def block_of(position):
        return (jnp.arange(values.shape[position]) // (values.shape[position] // shards_of)).reshape((-1,) + (1,) * (values.ndim - 1 - position))

    near = jax.random.permutation(rng, shards_of)[block_of(target)]
    other_side = (block_of(target) + shards_of // 2) % shards_of
    return jnp.where((block_of(source) == near) | (block_of(source) == other_side), factor * values, values)


def block_levels(key, shape, pieces, least, high):
    def one(dim, blocks):
        heights = jax.random.uniform(jax.random.fold_in(jax.random.fold_in(key, 6), dim), (blocks,), jnp.float32, least / len(pieces), high / len(pieces))
        return jnp.repeat(jnp.exp(heights), shape[dim] // blocks).reshape((-1,) + (1,) * (len(shape) - dim - 1))

    loudness = one(*pieces[0])
    for cut in pieces[1:]:
        loudness = loudness * one(*cut)
    return loudness


def normal_values(own_key, dims, spread, most, cuts=(), held_as=jnp.bfloat16):
    result = jax.random.normal(own_key, dims, jnp.float32) * spread
    if len(cuts) > 0:
        result = block_levels(own_key, dims, cuts, -0.22, 0.18) * result
    return jnp.clip(result, min=-most, max=most).astype(held_as)


def heavy_noise(own_key, extent, scale, reach, shards, heavy, dtype=jnp.bfloat16):
    array = scale * jax.random.normal(own_key, extent, jnp.float32)
    if shards:
        array = array * block_levels(own_key, extent, shards, -0.22, 0.18)
    return jnp.clip(spiked(array, jax.random.fold_in(own_key, 3), *heavy), -reach, reach).astype(dtype)


def setup_inputs(seed: int = 0) -> dict:
    seeds = jax.random.split(jax.random.key(seed), 9)
    return {
        "residual_in": draw_residual_in(jax.random.fold_in(seeds[8], 71), 0),
        "norm_gain": jnp.clip(1.0 + 0.18 * jax.random.normal(seeds[1], (LAYERS, D), jnp.float32), 0.1, 1.9),
        "gate_proj": normal_values(seeds[2], (LAYERS, D, CW), D ** -0.5, 0.09375, ((1, 16), (2, 16))),
        "filter_proj": normal_values(seeds[3], (LAYERS, D, CW), D ** -0.5, 0.09375, ((1, 16), (2, 16))),
        "signal_proj": normal_values(seeds[4], (LAYERS, D, CW), D ** -0.5, 0.09375, ((1, 16), (2, 16))),
        "conv_taps": normal_values(seeds[5], (LAYERS, TAPS, CW), 0.6, 3.0, ((2, 16),), jnp.float32),
        "out_proj": heavy_noise(seeds[6], (LAYERS, CW, D), CW ** -0.5, 0.1875, ((1, 16), (2, 16)), (1, 2, 16, 2.0)),
        "final_gain": jnp.clip(1.0 + 0.18 * jax.random.normal(seeds[7], (D,), jnp.float32), 0.1, 1.9),
    }


norm_floor = 1e-06

def rms_scaled(values, gain_row):
    mean_square = lax.optimization_barrier(jnp.mean(values * values, axis=-1, keepdims=True))
    return values * lax.rsqrt(mean_square + norm_floor) * gain_row

def stored(values):
    return lax.optimization_barrier(values.astype(jnp.bfloat16)).astype(jnp.float32)

def causal_filter(product, taps):
    width_taps = taps.shape[0]
    length = product.shape[0]
    padded = jnp.concatenate([jnp.zeros((width_taps - 1, product.shape[1]), jnp.bfloat16), product], axis=0)
    filtered = jnp.zeros(product.shape, jnp.float32)
    for tap_index in range(width_taps):
        filtered = filtered + taps[tap_index] * padded[tap_index:tap_index + length].astype(jnp.float32)
    return filtered

def reference(residual_in, norm_gain, gate_proj, filter_proj, signal_proj, conv_taps, out_proj, final_gain):
    stream = residual_in
    block_width = CW // N_TP
    for layer_number in range(LAYERS):
        normed = rms_scaled(stream.astype(jnp.float32), norm_gain[layer_number]).astype(jnp.bfloat16)
        gate_rows = stored(jnp.dot(normed, gate_proj[layer_number], preferred_element_type=jnp.float32))
        filter_in = stored(jnp.dot(normed, filter_proj[layer_number], preferred_element_type=jnp.float32))
        signal_rows = stored(jnp.dot(normed, signal_proj[layer_number], preferred_element_type=jnp.float32))
        product = (filter_in * signal_rows).astype(jnp.bfloat16)
        filtered = causal_filter(product, conv_taps[layer_number])
        mixed_rows = (gate_rows * filtered).astype(jnp.bfloat16)
        branch = jnp.zeros((mixed_rows.shape[0], D), jnp.float32)
        for block_number in range(N_TP):
            lower_col = block_number * block_width
            partial_sum = jnp.dot(mixed_rows[:, lower_col:lower_col + block_width], out_proj[layer_number, lower_col:lower_col + block_width], preferred_element_type=jnp.float32)
            branch = branch + stored(partial_sum)
        stream = (stream.astype(jnp.float32) + branch).astype(jnp.bfloat16)
    return rms_scaled(stream.astype(jnp.float32), final_gain)
```

```python
import jax
import jax.numpy as jnp
from jax import lax
from jax.experimental import pallas as pl
from jax.experimental.pallas import tpu as pltpu
from jax.sharding import PartitionSpec as P

D = 4096
TAPS = 3
LAYERS = 2
FLOOR = 1e-06

NZ = 8
SIDE = 4
ROWS = 256
PIECE = 512
CH = 128
WIDE = 512
NQ = 2
QR = ROWS // NQ

F32 = jnp.float32
BF16 = jnp.bfloat16
MESH = pl.DeviceIdType.MESH


def aligned(index, size):
    return pl.ds(pl.multiple_of(index * size, size), size)


def kernel(
    res, norm_gain, gate, filt, sig, taps, outp, final_gain, out,
    x_all, xg, w_all, w_out, acc, prod, mixed, sq, rs_out, rs_in, halo, tap_all, sums, st, fin_out, fin_in,
    ag_s, ag_r, w_s, w_r, d_s, d_r, rs_s, rs_r, h_s, h_r, s_s, s_r, m_s, m_r,
):
    s = lax.axis_index("sp")
    t = lax.axis_index("tp")
    z, c = t // 2, t % 2
    y, x = s // SIDE, s % SIDE
    other = 1 - c
    partner = (s, 2 * z + other)

    def at_z(k):
        return (s, ((z + k) % NZ) * 2 + c)

    def at_x(k):
        return (y * SIDE + (x + k) % SIDE, t)

    def at_y(k):
        return (((y + k) % SIDE) * SIDE + x, t)

    halo_next = ((s + c) % 16, 2 * z + other)
    halo_far = ((s + 2 * c + 15) % 16, 2 * z + other)

    def rdma(src, dst, send, recv, device):
        return pltpu.make_async_remote_copy(
            src_ref=src, dst_ref=dst, send_sem=send, recv_sem=recv, device_id=device, device_id_type=MESH
        )

    pending = []

    def start(copy):
        copy.start()
        pending.append(copy)

    barrier = pltpu.get_barrier_semaphore()
    peers = [at_z(k) for k in range(1, NZ)] + [at_x(1), at_x(-1), at_y(1), at_y(-1), partner, halo_far]
    for peer in peers:
        pl.semaphore_signal(barrier, inc=1, device_id=peer, device_id_type=MESH)

    own_cols = aligned(c, 256)
    own_rows = aligned(c, ROWS)
    other_rows = aligned(other, ROWS)
    own_wide = aligned(c, WIDE)

    x_all[0, z, :, own_cols] = res[own_rows, :]
    for l in range(LAYERS):
        for part, ref in enumerate((gate, filt, sig)):
            w_all[l, aligned(s, 256), pl.ds(pl.multiple_of(c * WIDE + part * CH, CH), CH)] = ref[l]
        for h in range(2):
            w_all[l, aligned(2 * s + h, CH), pl.ds(pl.multiple_of(c * WIDE + 3 * CH, CH), CH)] = outp[
                l, :, h * CH : (h + 1) * CH
            ]
    for l in range(LAYERS):
        for k in range(TAPS):
            tap_all[c, l * TAPS + k] = taps[l, k : k + 1, :]
    pl.semaphore_wait(barrier, len(peers))

    start(rdma(res.at[other_rows, :], x_all.at[0, z, :, own_cols], m_s.at[0], m_r.at[0], partner))
    start(rdma(tap_all.at[c], tap_all.at[c], m_s.at[1], m_r.at[1], partner))

    def piece(l, axis, along, across, lo, size):
        if axis == 0:
            yy, xx = y + across, x + along
        else:
            yy, xx = y + along, x + across
        index = ((yy + SIDE) % SIDE) * SIDE + (xx + SIDE) % SIDE
        return w_all.at[l, pl.ds(pl.multiple_of(index * 256 + lo, 64), size), own_wide]

    def w_copy(l, group, half, axis, across, sign, fwd, sending):
        step = sign if fwd else 0
        along = -step if sending else -step - sign
        lo, size = half * 128, 128
        if fwd:
            lo, size = lo + (0 if sign == 1 else 64), 64
        slot = group * 4 + (2 if fwd else 0) + (0 if sign == 1 else 1)
        ref = piece(l, axis, along, across, lo, size)
        device = at_x(sign) if axis == 0 else at_y(sign)
        return rdma(ref, ref, w_s.at[l, slot], w_r.at[l, slot], device)

    groups = {("a", 1): (0, 0, 0, 0), ("b", 1): (5, 1, 1, 0)}
    for i, p in enumerate((0, -1, 1, 2)):
        groups["a", 2, p] = (1 + i, 0, 1, p)
        groups["b", 2, p] = (6 + i, 1, 0, p)

    def w_send(l, *name):
        group, half, axis, across = groups[name]
        for sign in (1, -1):
            start(w_copy(l, group, half, axis, across, sign, False, True))

    def w_forward(l, *name):
        group, half, axis, across = groups[name]
        for sign in (1, -1):
            w_copy(l, group, half, axis, across, sign, False, False).wait_recv()
            start(w_copy(l, group, half, axis, across, sign, True, True))

    def w_finish(l, *name):
        group, half, axis, across = groups[name]
        for sign in (1, -1):
            w_copy(l, group, half, axis, across, sign, True, False).wait_recv()

    def w_row(l, k, core):
        return w_all.at[l, aligned((y + k + SIDE) % SIDE, 1024), aligned(core, WIDE)]

    def w_hand(l, k):
        slot = (k + SIDE) % SIDE
        start(rdma(w_row(l, k, c), w_row(l, k, c), d_s.at[l, slot], d_r.at[l, slot], partner))

    def w_taken(l, k):
        slot = (k + SIDE) % SIDE
        rdma(w_row(l, k, other), w_row(l, k, other), d_s.at[l, slot], d_r.at[l, slot], partner).wait_recv()

    def w_stage(l, stage):
        if stage == 0:
            w_send(l, "a", 1)
            w_send(l, "b", 1)
            w_send(l, "b", 2, 0)
            w_send(l, "a", 2, 0)
        elif stage == 1:
            w_forward(l, "a", 1)
            w_forward(l, "b", 1)
            for p in (-1, 1):
                w_send(l, "a", 2, p)
                w_send(l, "b", 2, p)
        elif stage == 2:
            w_forward(l, "b", 2, 0)
            w_forward(l, "a", 2, 0)
            w_finish(l, "a", 1)
            w_send(l, "a", 2, 2)
            w_finish(l, "b", 1)
            w_send(l, "b", 2, 2)
        elif stage == 3:
            for p in (-1, 1):
                w_forward(l, "a", 2, p)
                w_forward(l, "b", 2, p)
            w_finish(l, "a", 2, 0)
            w_finish(l, "b", 2, 0)
            w_hand(l, 0)
        elif stage == 4:
            w_forward(l, "a", 2, 2)
            w_forward(l, "b", 2, 2)
            for p in (-1, 1):
                w_finish(l, "a", 2, p)
                w_finish(l, "b", 2, p)
            w_hand(l, -1)
            w_hand(l, 1)
        elif stage == 5:
            w_finish(l, "a", 2, 2)
            w_finish(l, "b", 2, 2)
            w_hand(l, 2)
        else:
            for k in (0, -1, 1, 2):
                w_taken(l, k)

    def build_w_out(l):
        def body(i, carry):
            for core in range(2):
                w_out[core * CH : (core + 1) * CH, aligned(i, CH)] = w_all[
                    l, aligned(i, CH), core * WIDE + 3 * CH : (core + 1) * WIDE
                ]
            return carry

        lax.fori_loop(0, D // CH, body, 0)

    def ag_has(way, dist, q):
        return dist < 3 or (q < NQ // 2) == (way == 0)

    def ag_copy(l, way, dist, q, sending):
        sign = 1 - 2 * way
        chunk = (z - sign * (dist if sending else dist + 1) + NZ) % NZ
        ref = x_all.at[l, chunk, pl.ds(q * QR, QR), :]
        return rdma(ref, ref, ag_s.at[l, way, dist * NQ + q], ag_r.at[l, way, dist * NQ + q], at_z(sign))

    def ag_send(l, dist, q):
        for way in range(2):
            if ag_has(way, dist, q):
                start(ag_copy(l, way, dist, q, True))

    def ag_step(l, dist, q):
        for way in range(2):
            if ag_has(way, dist, q):
                ag_copy(l, way, dist, q, False).wait_recv()
                if dist < 3 and ag_has(way, dist + 1, q):
                    start(ag_copy(l, way, dist + 1, q, True))

    def take(l, chunk):
        value = x_all[l, chunk].astype(F32)
        square = value * value
        total = square[:, :128]
        for i in range(1, PIECE // 128):
            total = total + square[:, i * 128 : (i + 1) * 128]
        sq[...] += total
        xg[chunk] = (value * norm_gain[l : l + 1, aligned(chunk, PIECE)]).astype(BF16)

    def multiply(l, chunk):
        rows = aligned(chunk, PIECE)
        for core in range(2):
            cols = pl.ds(core * 3 * CH, 3 * CH)
            acc[:, cols] += jnp.dot(
                xg[chunk], w_all[l, rows, core * WIDE : core * WIDE + 3 * CH], preferred_element_type=F32
            )

    def start_sums():
        sq[...] = jnp.zeros_like(sq)
        acc[...] = jnp.zeros_like(acc)

    def chunk_at(k):
        return (z + k + NZ) % NZ

    def mix(l, lo, size):
        rows = pl.ds(lo, size)
        for core in range(2):
            cols = pl.ds(core * CH, CH)
            filtered = jnp.zeros((size, CH), F32)
            for k in range(TAPS):
                filtered = filtered + tap_all[core, l * TAPS + k] * prod[pl.ds(8 + lo - (TAPS - 1) + k, size), cols]
            gated = acc[rows, core * 3 * CH : core * 3 * CH + CH]
            mixed[rows, cols] = (gated * filtered).astype(BF16)

    def gates(l):
        mean = jnp.sum(sq[...], axis=1, keepdims=True) / D
        scale = lax.rsqrt(mean + FLOOR)
        for core in range(2):
            base = core * 3 * CH
            value = (acc[:, base + CH : base + 2 * CH] * scale) * (acc[:, base + 2 * CH : base + 3 * CH] * scale)
            prod[8:, core * CH : (core + 1) * CH] = value.astype(BF16).astype(F32)
            acc[:, base : base + CH] = acc[:, base : base + CH] * scale
        halo[l, 0] = prod[ROWS:, :]

    def halo_copy(l):
        return rdma(halo.at[l, 0], halo.at[l, 1], h_s.at[l], h_r.at[l], halo_next)

    def take_halo(l):
        halo_copy(l).wait_recv()
        first = jnp.logical_and(s == 0, c == 0)
        prod[:8, :] = jnp.where(first, 0.0, halo[l, 1])

    def rs_has(way, k, q):
        return k < 4 or (q < NQ // 2) == (way == 0)

    def rs_copy(l, way, k, q):
        slot = (k - 1) * NQ + q
        return rdma(
            rs_out.at[l, way, slot], rs_in.at[l, way, slot], rs_s.at[l, way, slot], rs_r.at[l, way, slot],
            at_z(1 - 2 * way),
        )

    def partial(q, chunk):
        return jnp.dot(mixed[q * QR : (q + 1) * QR, :], w_out[:, aligned(chunk, PIECE)], preferred_element_type=F32)

    def arrived(l, way, k, q):
        rs_copy(l, way, k, q).wait_recv()
        return rs_in[l, way, (k - 1) * NQ + q].astype(F32)

    def rs_step(l, i, q):
        for way in range(2):
            k = 4 - i if rs_has(way, 4, q) else 3 - i
            if k < 1:
                continue
            value = partial(q, chunk_at(k * (1 - 2 * way)))
            if i > 0:
                value = value + arrived(l, way, k + 1, q)
            rs_out[l, way, (k - 1) * NQ + q] = value.astype(BF16)
            start(rs_copy(l, way, k, q))

    def rs_last(l, q):
        value = partial(q, z)
        for way in range(2):
            value = value + arrived(l, way, 1, q)
        return (x_all[l, z, pl.ds(q * QR, QR), :].astype(F32) + value).astype(BF16)

    upper = list(range(NQ // 2, NQ))
    lower = list(range(NQ // 2))

    start_sums()
    rdma(res.at[other_rows, :], x_all.at[0, z, :, aligned(other, 256)], m_s.at[0], m_r.at[0], partner).wait_recv()
    for q in range(NQ):
        ag_send(0, 0, q)
    w_stage(0, 0)
    take(0, z)
    for dist in range(4):
        for q in range(NQ):
            ag_step(0, dist, q)
            if q == NQ // 2 - 1:
                w_stage(0, (1, 1, 3, 4)[dist]) if dist != 1 else None
        if dist == 0:
            w_stage(0, 2)
        if dist < 3:
            take(0, chunk_at(-dist - 1))
            take(0, chunk_at(dist + 1))
        else:
            take(0, chunk_at(4))
    w_stage(0, 5)
    w_stage(1, 0)
    rdma(tap_all.at[other], tap_all.at[other], m_s.at[1], m_r.at[1], partner).wait_recv()
    w_stage(0, 6)

    def all_blocks(i, carry):
        multiply(0, i)
        return carry

    lax.fori_loop(0, NZ, all_blocks, 0)

    for l in range(LAYERS):
        gates(l)
        start(halo_copy(l))
        build_w_out(l)
        mix(l, ROWS // 2, ROWS // 2)
        for i in range(4):
            for q in upper:
                rs_step(l, i, q)
            if i == 0:
                take_halo(l)
                mix(l, 0, ROWS // 2)
            for q in lower:
                rs_step(l, i, q)
            if l == 0:
                w_stage(1, 1 + i)
        if l == 0:
            start_sums()
            for q in upper + lower:
                x_all[1, z, pl.ds(q * QR, QR), :] = rs_last(0, q)
                ag_send(1, 0, q)
            w_stage(1, 5)
            take(1, z)
            w_stage(1, 6)
            multiply(1, z)
            for dist in range(4):
                for q in upper + lower:
                    ag_step(1, dist, q)
                for k in (-dist - 1, dist + 1) if dist < 3 else (4,):
                    take(1, chunk_at(k))
                    multiply(1, chunk_at(k))

    for q in upper + lower:
        value = rs_last(1, q).astype(F32)
        st[pl.ds(q * QR, QR), :] = value
    value = st[...]
    square = jnp.sum(value * value, axis=1, keepdims=True)
    sums[z] = jnp.broadcast_to(square, (ROWS, 128)).T[:8, :]

    def sums_copy(k, sending):
        ref = sums.at[z if sending else chunk_at(-k)]
        return rdma(ref, ref, s_s.at[k], s_r.at[k], at_z(k))

    for k in (4, 3, 5, 2, 6, 1, 7):
        start(sums_copy(k, True))
    total = sums[z]
    for k in (1, 7, 2, 6, 3, 5, 4):
        sums_copy(k, False).wait_recv()
        total = total + sums[chunk_at(-k)]
    total = jnp.broadcast_to(total[:1, :], (128, ROWS)).T[:, :1]
    scale = lax.rsqrt(total / D + FLOOR)
    fin_out[...] = st[:, aligned(other, 256)] * scale
    back = rdma(fin_out, fin_in, m_s.at[2], m_r.at[2], partner)
    start(back)
    out[own_rows, :] = st[:, own_cols] * scale * final_gain[...]
    back.wait_recv()
    out[other_rows, :] = fin_in[...] * final_gain[...]
    for copy in pending:
        copy.wait_send()


def per_device(residual_in, norm_gain, gate_proj, filter_proj, signal_proj, conv_taps, out_proj, final_gain):
    vmem = pl.BlockSpec(memory_space=pltpu.VMEM)
    dma = pltpu.SemaphoreType.DMA
    return pl.pallas_call(
        kernel,
        out_shape=jax.ShapeDtypeStruct((2 * ROWS, 256), F32),
        in_specs=[vmem] * 8,
        out_specs=vmem,
        scratch_shapes=[
            pltpu.VMEM((LAYERS, NZ, ROWS, PIECE), BF16),
            pltpu.VMEM((NZ, ROWS, PIECE), BF16),
            pltpu.VMEM((LAYERS, D, 2 * WIDE), BF16),
            pltpu.VMEM((2 * CH, D), BF16),
            pltpu.VMEM((ROWS, 6 * CH), F32),
            pltpu.VMEM((8 + ROWS, 2 * CH), F32),
            pltpu.VMEM((ROWS, 2 * CH), BF16),
            pltpu.VMEM((ROWS, 128), F32),
            pltpu.VMEM((LAYERS, 2, 4 * NQ, QR, PIECE), BF16),
            pltpu.VMEM((LAYERS, 2, 4 * NQ, QR, PIECE), BF16),
            pltpu.VMEM((LAYERS, 2, 8, 2 * CH), F32),
            pltpu.VMEM((2, LAYERS * TAPS, 1, CH), F32),
            pltpu.VMEM((NZ, 8, ROWS), F32),
            pltpu.VMEM((ROWS, PIECE), F32),
            pltpu.VMEM((ROWS, 256), F32),
            pltpu.VMEM((ROWS, 256), F32),
            dma((LAYERS, 2, 4 * NQ)), dma((LAYERS, 2, 4 * NQ)),
            dma((LAYERS, 40)), dma((LAYERS, 40)),
            dma((LAYERS, SIDE)), dma((LAYERS, SIDE)),
            dma((LAYERS, 2, 4 * NQ)), dma((LAYERS, 2, 4 * NQ)),
            dma((LAYERS,)), dma((LAYERS,)),
            dma((NZ,)), dma((NZ,)),
            dma((3,)), dma((3,)),
        ],
        compiler_params=pltpu.CompilerParams(
            collective_id=0, has_side_effects=True, vmem_limit_bytes=58 * 1024 * 1024
        ),
    )(
        residual_in, norm_gain, gate_proj, filter_proj, signal_proj, conv_taps, out_proj,
        final_gain.reshape(1, -1),
    )


def solution(mesh):
    return jax.shard_map(
        per_device,
        mesh=mesh,
        in_specs=(
            P("sp", "tp"),
            P(),
            P(None, "sp", "tp"),
            P(None, "sp", "tp"),
            P(None, "sp", "tp"),
            P(None, None, "tp"),
            P(None, "tp", "sp"),
            P("tp"),
        ),
        out_specs=P("sp", "tp"),
        check_vma=False,
    )
```

```python
import jax
import jax.numpy as jnp
from jax import lax
from jax.experimental import pallas as pl
from jax.experimental.pallas import tpu as pltpu
from jax.sharding import PartitionSpec as P

D = 4096
TAPS = 3
LAYERS = 2
FLOOR = 1e-06

NZ = 8
SIDE = 4
ROWS = 256
PIECE = 512
COLS = 256
CH = 128
WIDE = 512

F32 = jnp.float32
BF16 = jnp.bfloat16
MESH = pl.DeviceIdType.MESH

GATHER = (((96, 80), (176, 80), (0, 48), (48, 48)), ((112, 80), (192, 64), (0, 64), (64, 48)))
REDUCE = (((112, 80), (192, 64), (0, 64), (64, 48)), ((128, 64), (192, 64), (0, 64), (64, 64)))
GROUPS = ((0, 1), (2, 3))


def span(units, group):
    lo = units[GROUPS[group][0]][0]
    return lo, sum(units[u][1] for u in GROUPS[group])


def aligned(index, size):
    return pl.ds(pl.multiple_of(index * size, size), size)


def has(way, far, unit):
    return not far or (unit % 2 == 0) == (way == 0)


def kernel(
    res, norm_gain, gate, filt, sig, taps, outp, final_gain, out,
    x_all, res_other, xg, w_all, w_out, acc, prod, mixed, sq, rs_out, rs_in, halo, tap_all, gain_in, gain_out,
    sums, st, fin_out, fin_in,
    loc, ag0_s, ag0_r, ag_s, ag_r, w_s, w_r, d_s, d_r, rs_s, rs_r, h_s, h_r, s_s, s_r, m_s, m_r,
):
    s = lax.axis_index("sp")
    t = lax.axis_index("tp")
    z, c = t // 2, t % 2
    y, x = s // SIDE, s % SIDE
    other = 1 - c
    partner = (s, 2 * z + other)

    def at_z(k, core=None):
        return (s, ((z + k + NZ) % NZ) * 2 + (c if core is None else core))

    def at_x(k):
        return (y * SIDE + (x + k + SIDE) % SIDE, t)

    def at_y(k):
        return (((y + k + SIDE) % SIDE) * SIDE + x, t)

    halo_next = ((s + c) % 16, 2 * z + other)
    halo_far = ((s + 2 * c + 15) % 16, 2 * z + other)

    def rdma(src, dst, send, recv, device):
        return pltpu.make_async_remote_copy(
            src_ref=src, dst_ref=dst, send_sem=send, recv_sem=recv, device_id=device, device_id_type=MESH
        )

    pending = []

    def start(copy):
        copy.start()
        pending.append(copy)

    barrier = pltpu.get_barrier_semaphore()
    peers = [at_z(1), at_z(-1), at_z(1, other), at_z(-1, other), at_x(1), at_x(-1), at_y(1), at_y(-1), partner]
    for peer in peers:
        pl.semaphore_signal(barrier, inc=1, device_id=peer, device_id_type=MESH)

    own_cols = aligned(c, COLS)
    other_cols = aligned(other, COLS)
    own_rows = aligned(c, ROWS)
    other_rows = aligned(other, ROWS)
    own_wide = aligned(c, WIDE)

    local = []

    def place(src, dst):
        copy = pltpu.make_async_copy(src, dst, loc.at[len(local)])
        copy.start()
        local.append(copy)

    place(res.at[own_rows, :], x_all.at[0, z, :, own_cols])
    place(res.at[other_rows, :], res_other)
    for l in range(LAYERS):
        for part, ref in enumerate((gate, filt, sig)):
            first = pl.multiple_of(c * 3 * CH + (part + 1) * CH, CH)
            place(ref.at[l], w_all.at[l, aligned(s, 256), pl.ds(first, CH)])
        for h in range(2):
            place(
                outp.at[l, :, pl.ds(h * CH, CH)],
                w_all.at[l, aligned(2 * s + h, CH), aligned(c * 7, CH)],
            )
    place(norm_gain, gain_in)
    place(taps, tap_all.at[c])
    place(final_gain, gain_out)

    with jax.named_scope("barrier"):
        pl.semaphore_wait(barrier, len(peers))
    with jax.named_scope("local"):
        for copy in local:
            copy.wait()

    def piece(l, axis, along, across, lo, size):
        if axis == 0:
            yy, xx = y + across, x + along
        else:
            yy, xx = y + along, x + across
        index = ((yy + SIDE) % SIDE) * SIDE + (xx + SIDE) % SIDE
        return w_all.at[l, pl.ds(pl.multiple_of(index * 256 + lo, 64), size), own_wide]

    def w_copy(l, group, half, axis, across, sign, fwd, sending):
        step = sign if fwd else 0
        along = -step if sending else -step - sign
        lo, size = half * 128, 128
        if fwd:
            lo, size = lo + (0 if sign == 1 else 64), 64
        slot = group * 4 + (2 if fwd else 0) + (0 if sign == 1 else 1)
        ref = piece(l, axis, along, across, lo, size)
        device = at_x(sign) if axis == 0 else at_y(sign)
        return rdma(ref, ref, w_s.at[l, slot], w_r.at[l, slot], device)

    groups = {("a", 1): (0, 0, 0, 0), ("b", 1): (5, 1, 1, 0)}
    for i, p in enumerate((0, -1, 1, 2)):
        groups["a", 2, p] = (1 + i, 0, 1, p)
        groups["b", 2, p] = (6 + i, 1, 0, p)

    def w_send(l, *name):
        group, half, axis, across = groups[name]
        for sign in (1, -1):
            start(w_copy(l, group, half, axis, across, sign, False, True))

    def w_forward(l, *name):
        group, half, axis, across = groups[name]
        for sign in (1, -1):
            w_copy(l, group, half, axis, across, sign, False, False).wait_recv()
            start(w_copy(l, group, half, axis, across, sign, True, True))

    def w_finish(l, *name):
        group, half, axis, across = groups[name]
        for sign in (1, -1):
            w_copy(l, group, half, axis, across, sign, True, False).wait_recv()

    def w_row(l, k, core):
        return w_all.at[l, aligned((y + k + SIDE) % SIDE, 1024), aligned(core, WIDE)]

    def w_hand(l, k):
        slot = (k + SIDE) % SIDE
        start(rdma(w_row(l, k, c), w_row(l, k, c), d_s.at[l, slot], d_r.at[l, slot], partner))

    def w_taken(l, k):
        slot = (k + SIDE) % SIDE
        with jax.named_scope(f"taken#l={l}#k={k}"):
            rdma(w_row(l, k, other), w_row(l, k, other), d_s.at[l, slot], d_r.at[l, slot], partner).wait_recv()

    def w_stage(l, stage):
        with jax.named_scope(f"w#l={l}#s={stage}"):
            w_stage_body(l, stage)

    def w_stage_body(l, stage):
        if stage == 0:
            w_send(l, "a", 1)
            w_send(l, "b", 1)
            w_send(l, "b", 2, 0)
            w_send(l, "a", 2, 0)
        elif stage == 1:
            w_forward(l, "a", 1)
            w_forward(l, "b", 1)
            for p in (-1, 1):
                w_send(l, "a", 2, p)
                w_send(l, "b", 2, p)
        elif stage == 2:
            w_forward(l, "b", 2, 0)
            w_forward(l, "a", 2, 0)
            w_finish(l, "a", 1)
            w_send(l, "a", 2, 2)
            w_finish(l, "b", 1)
            w_send(l, "b", 2, 2)
        elif stage == 3:
            for p in (-1, 1):
                w_forward(l, "a", 2, p)
                w_forward(l, "b", 2, p)
            w_finish(l, "a", 2, 0)
            w_finish(l, "b", 2, 0)
            w_hand(l, 0)
        elif stage == 4:
            w_forward(l, "a", 2, 2)
            w_forward(l, "b", 2, 2)
            for p in (-1, 1):
                w_finish(l, "a", 2, p)
                w_finish(l, "b", 2, p)
            w_hand(l, -1)
            w_hand(l, 1)
        else:
            w_finish(l, "a", 2, 2)
            w_finish(l, "b", 2, 2)
            w_hand(l, 2)

    def build_w_out(l, k):
        first = ((y + k + SIDE) % SIDE) * 8

        def body(i, carry):
            for core in range(2):
                w_out[core * CH : (core + 1) * CH, aligned(first + i, CH)] = w_all[
                    l, aligned(first + i, CH), core * 7 * CH : (core * 7 + 1) * CH
                ]
            return carry

        lax.fori_loop(0, 8, body, 0)

    def chunk_at(k):
        return (z + k + NZ) % NZ

    def ag_copy(l, way, dist, unit, sending):
        sign = 1 - 2 * way
        lo, size = GATHER[l][unit]
        ref = x_all.at[l, chunk_at(-sign * (dist if sending else dist + 1)), pl.ds(lo, size), :]
        slot = dist * 4 + unit
        return rdma(ref, ref, ag_s.at[l, way, slot], ag_r.at[l, way, slot], at_z(sign))

    def first_copy(way, unit, crossing, sending):
        sign = 1 - 2 * way
        lo, size = GATHER[0][unit]
        cols = own_cols if sending or not crossing else other_cols
        dst = x_all.at[0, z if sending else chunk_at(-sign), pl.ds(lo, size), cols]
        src = res_other.at[pl.ds(lo, size), :] if crossing else x_all.at[0, z, pl.ds(lo, size), own_cols]
        slot = unit * 2 + (1 if crossing else 0)
        return rdma(src, dst, ag0_s.at[way, slot], ag0_r.at[way, slot], at_z(sign, other if crossing else c))

    def ag_first(l, unit):
        for way in range(2):
            if l == 0:
                start(first_copy(way, unit, False, True))
                start(first_copy(way, unit, True, True))
            else:
                start(ag_copy(l, way, 0, unit, True))

    def ag_step(l, dist, unit):
        with jax.named_scope(f"ag#l={l}#d={dist}#u={unit}"):
            for way in range(2):
                if not has(way, dist == 3, unit):
                    continue
                if l == 0 and dist == 0:
                    first_copy(way, unit, False, False).wait_recv()
                    first_copy(way, unit, True, False).wait_recv()
                else:
                    ag_copy(l, way, dist, unit, False).wait_recv()
                if dist < 3 and has(way, dist == 2, unit):
                    start(ag_copy(l, way, dist + 1, unit, True))

    def take(l, group, chunk):
        lo, size = span(GATHER[l], group)
        rows = pl.ds(lo, size)
        value = x_all[l, chunk, rows, :].astype(F32)
        square = value * value
        total = square[:, :128]
        for i in range(1, PIECE // 128):
            total = total + square[:, i * 128 : (i + 1) * 128]
        sq[rows, :] += total
        xg[chunk, rows, :] = (value * gain_in[l : l + 1, aligned(chunk, PIECE)]).astype(BF16)

    def arrived_at(dist):
        return (-dist - 1, dist + 1) if dist < 3 else (4,)

    def multiply(l, group, chunk):
        lo, size = span(GATHER[l], group)
        acc[lo : lo + size, :] += jnp.dot(
            xg[chunk, lo : lo + size, :],
            w_all[l, aligned(chunk, PIECE), CH : 7 * CH],
            preferred_element_type=F32,
        )

    def multiply_row(l, group, k):
        first = ((y + k + SIDE) % SIDE) * 2
        with jax.named_scope(f"mult#g={group}"):
            multiply(l, group, first)
            multiply(l, group, first + 1)

    def start_sums():
        sq[...] = jnp.zeros_like(sq)
        acc[...] = jnp.zeros_like(acc)

    def gates(l, group):
        lo, size = span(GATHER[l], group)
        rows = pl.ds(lo, size)
        mean = jnp.sum(sq[rows, :], axis=1, keepdims=True) / D
        scale = lax.rsqrt(mean + FLOOR)
        for core in range(2):
            base = core * 3 * CH
            value = (acc[rows, base + CH : base + 2 * CH] * scale) * (acc[rows, base + 2 * CH : base + 3 * CH] * scale)
            prod[pl.ds(8 + lo, size), core * CH : (core + 1) * CH] = value.astype(BF16).astype(F32)
            acc[rows, base : base + CH] = acc[rows, base : base + CH] * scale

    def mix(l, group):
        lo, size = span(REDUCE[l], group)
        rows = pl.ds(lo, size)
        for core in range(2):
            cols = pl.ds(core * CH, CH)
            filtered = jnp.zeros((size, CH), F32)
            for k in range(TAPS):
                tap = tap_all[core, k, l : l + 1, :]
                filtered = filtered + tap * prod[pl.ds(8 + lo - (TAPS - 1) + k, size), cols]
            gated = acc[rows, core * 3 * CH : core * 3 * CH + CH]
            mixed[rows, cols] = (gated * filtered).astype(BF16)

    def halo_copy(l):
        return rdma(halo.at[l, 0], halo.at[l, 1], h_s.at[l], h_r.at[l], halo_next)

    def give_halo(l):
        halo[l, 0] = prod[ROWS:, :]
        start(halo_copy(l))

    def take_halo(l):
        with jax.named_scope("halo"):
            halo_copy(l).wait_recv()
        first = jnp.logical_and(s == 0, c == 0)
        prod[:8, :] = jnp.where(first, 0.0, halo[l, 1])

    def rs_copy(l, way, k, unit):
        lo, size = REDUCE[l][unit]
        rows = pl.ds(lo, size)
        slot = (k - 1) * 4 + unit
        return rdma(
            rs_out.at[l, way, k - 1, rows, :], rs_in.at[l, way, k - 1, rows, :],
            rs_s.at[l, way, slot], rs_r.at[l, way, slot], at_z(1 - 2 * way),
        )

    def partial(l, unit, chunk):
        lo, size = REDUCE[l][unit]
        return jnp.dot(mixed[lo : lo + size, :], w_out[:, aligned(chunk, PIECE)], preferred_element_type=F32)

    def arrived(l, way, k, unit):
        rs_copy(l, way, k, unit).wait_recv()
        lo, size = REDUCE[l][unit]
        return rs_in[l, way, k - 1, lo : lo + size, :].astype(F32)

    def rs_step(l, i, group):
        for unit in GROUPS[group][::-1]:
            with jax.named_scope(f"rs#l={l}#i={i}#u={unit}"):
                lo, size = REDUCE[l][unit]
                for way in range(2):
                    k = 4 - i if has(way, True, unit) else 3 - i
                    if k < 1:
                        continue
                    value = partial(l, unit, chunk_at(k * (1 - 2 * way)))
                    if i > 0:
                        value = value + arrived(l, way, k + 1, unit)
                    rs_out[l, way, k - 1, lo : lo + size, :] = value.astype(BF16)
                    start(rs_copy(l, way, k, unit))

    def rs_last(l, unit):
        with jax.named_scope(f"last#l={l}#u={unit}"):
            lo, size = REDUCE[l][unit]
            value = partial(l, unit, z)
            for way in range(2):
                value = value + arrived(l, way, 1, unit)
            return (x_all[l, z, lo : lo + size, :].astype(F32) + value).astype(BF16)

    ag_first(0, 0)
    ag_first(0, 1)
    w_stage(0, 0)
    start(rdma(res_other, x_all.at[0, z, :, own_cols], m_s.at[0], m_r.at[0], partner))
    start(rdma(tap_all.at[c], tap_all.at[c], m_s.at[1], m_r.at[1], partner))
    ag_first(0, 2)
    ag_first(0, 3)
    start_sums()
    own_block = rdma(res_other, x_all.at[0, z, :, other_cols], m_s.at[0], m_r.at[0], partner)
    own_block.wait_recv()
    take(0, 0, z)
    take(0, 1, z)

    ag_step(0, 0, 0)
    w_stage(0, 1)
    ag_step(0, 0, 1)
    for k in arrived_at(0):
        take(0, 0, chunk_at(k))
    w_stage(0, 2)
    ag_step(0, 0, 2)
    ag_step(0, 0, 3)
    for k in arrived_at(0):
        take(0, 1, chunk_at(k))
    ag_step(0, 1, 0)
    ag_step(0, 1, 1)
    w_stage(0, 3)
    for k in arrived_at(1):
        take(0, 0, chunk_at(k))
    ag_step(0, 1, 2)
    ag_step(0, 1, 3)
    for k in arrived_at(1):
        take(0, 1, chunk_at(k))
    ag_step(0, 2, 0)
    ag_step(0, 2, 1)
    for k in arrived_at(2):
        take(0, 0, chunk_at(k))
    w_stage(0, 4)
    ag_step(0, 2, 2)
    ag_step(0, 2, 3)
    for k in arrived_at(2):
        take(0, 1, chunk_at(k))
    ag_step(0, 3, 0)
    ag_step(0, 3, 1)
    take(0, 0, chunk_at(4))
    w_taken(0, 0)
    multiply_row(0, 0, 0)
    w_stage(0, 5)
    w_stage(1, 0)
    for k in (-1, 1):
        w_taken(0, k)
        multiply_row(0, 0, k)
    ag_step(0, 3, 2)
    ag_step(0, 3, 3)
    take(0, 1, chunk_at(4))
    for k in (0, -1, 1):
        build_w_out(0, k)
    w_taken(0, 2)
    multiply_row(0, 0, 2)
    build_w_out(0, 2)
    rdma(tap_all.at[other], tap_all.at[other], m_s.at[1], m_r.at[1], partner).wait_recv()

    gates(0, 0)
    give_halo(0)
    mix(0, 0)
    rs_step(0, 0, 0)
    for k in (0, -1, 1, 2):
        multiply_row(0, 1, k)
    gates(0, 1)
    take_halo(0)
    mix(0, 1)
    rs_step(0, 0, 1)
    for i in (1, 2, 3):
        w_stage(1, i)
        rs_step(0, i, 0)
        rs_step(0, i, 1)
    start_sums()
    for group in range(2):
        for unit in GROUPS[group]:
            lo, size = REDUCE[0][unit]
            x_all[1, z, lo : lo + size, :] = rs_last(0, unit)
            ag_first(1, unit)
    w_stage(1, 4)
    w_stage(1, 5)
    for group in range(2):
        take(1, group, z)
    for k in (0, -1, 1, 2):
        w_taken(1, k)
        build_w_out(1, k)
    for group in range(2):
        multiply(1, group, z)
    for dist in range(3):
        for group in range(2):
            for unit in GROUPS[group]:
                ag_step(1, dist, unit)
            for k in arrived_at(dist):
                take(1, group, chunk_at(k))
                multiply(1, group, chunk_at(k))
    for group in range(2):
        for unit in GROUPS[group]:
            ag_step(1, 3, unit)
        take(1, group, chunk_at(4))
        multiply(1, group, chunk_at(4))
        gates(1, group)
        if group == 0:
            give_halo(1)
        else:
            take_halo(1)
        mix(1, group)
        rs_step(1, 0, group)
    for i in (1, 2, 3):
        rs_step(1, i, 0)
        rs_step(1, i, 1)

    def fin_copy(group):
        rows = pl.ds(*span(REDUCE[1], group))
        return rdma(fin_out.at[rows, :], fin_in.at[rows, :], m_s.at[2 + group], m_r.at[2 + group], partner)

    def sums_copy(group, k, crossing, sending):
        cols = pl.ds(*span(REDUCE[1], group))
        core = other if crossing and not sending else c
        ref = sums.at[core, z if sending else chunk_at(-k), :, cols]
        slot = 2 * k + (1 if crossing else 0)
        return rdma(ref, ref, s_s.at[group, slot], s_r.at[group, slot], at_z(k, other if crossing else c))

    routes = [(4, 0), (4, 1), (3, 0), (3, 1), (5, 0), (5, 1), (2, 0), (2, 1), (6, 0), (6, 1)]
    routes += [(1, 0), (1, 1), (7, 0), (7, 1), (0, 1)]
    for group in range(2):
        for unit in GROUPS[group]:
            lo, size = REDUCE[1][unit]
            st[lo : lo + size, :] = rs_last(1, unit).astype(F32)
        lo, size = span(REDUCE[1], group)
        rows = pl.ds(lo, size)
        value = st[rows, :]
        square = jnp.sum(value * value, axis=1, keepdims=True)
        sums[c, z, :, lo : lo + size] = jnp.broadcast_to(square, (size, 128)).T[:8, :]
        for k, crossing in routes:
            start(sums_copy(group, k, crossing, True))
        fin_out[rows, :] = st[rows, other_cols].astype(BF16)
        start(fin_copy(group))

    def scale_of(core):
        total = jnp.sum(sums[core, :, 0, :], axis=0, keepdims=True)
        return lax.rsqrt(jnp.broadcast_to(total, (128, ROWS)).T[:, :1] / D + FLOOR)

    with jax.named_scope("sums"):
        for group in range(2):
            fin_copy(group).wait_recv()
            for k, crossing in routes[::-1]:
                sums_copy(group, k, crossing, False).wait_recv()
    out[own_rows, :] = st[:, own_cols] * scale_of(c) * gain_out[...]
    out[other_rows, :] = fin_in[...].astype(F32) * scale_of(other) * gain_out[...]
    with jax.named_scope("sends"):
        for copy in pending:
            copy.wait_send()


def per_device(residual_in, norm_gain, gate_proj, filter_proj, signal_proj, conv_taps, out_proj, final_gain):
    dma = pltpu.SemaphoreType.DMA
    return pl.pallas_call(
        kernel,
        out_shape=jax.ShapeDtypeStruct((2 * ROWS, COLS), F32),
        in_specs=[pl.BlockSpec(memory_space=pltpu.HBM)] * 8,
        out_specs=pl.BlockSpec(memory_space=pltpu.VMEM),
        scratch_shapes=[
            pltpu.VMEM((LAYERS, NZ, ROWS, PIECE), BF16),
            pltpu.VMEM((ROWS, COLS), BF16),
            pltpu.VMEM((NZ, ROWS, PIECE), BF16),
            pltpu.VMEM((LAYERS, D, 2 * WIDE), BF16),
            pltpu.VMEM((2 * CH, D), BF16),
            pltpu.VMEM((ROWS, 6 * CH), F32),
            pltpu.VMEM((8 + ROWS, 2 * CH), F32),
            pltpu.VMEM((ROWS, 2 * CH), BF16),
            pltpu.VMEM((ROWS, 128), F32),
            pltpu.VMEM((LAYERS, 2, 4, ROWS, PIECE), BF16),
            pltpu.VMEM((LAYERS, 2, 4, ROWS, PIECE), BF16),
            pltpu.VMEM((LAYERS, 2, 8, 2 * CH), F32),
            pltpu.VMEM((2, TAPS, LAYERS, CH), F32),
            pltpu.VMEM((LAYERS, D), F32),
            pltpu.VMEM((1, COLS), F32),
            pltpu.VMEM((2, NZ, 8, ROWS), F32),
            pltpu.VMEM((ROWS, PIECE), F32),
            pltpu.VMEM((ROWS, COLS), BF16),
            pltpu.VMEM((ROWS, COLS), BF16),
            dma((16,)),
            dma((2, 8)), dma((2, 8)),
            dma((LAYERS, 2, 16)), dma((LAYERS, 2, 16)),
            dma((LAYERS, 40)), dma((LAYERS, 40)),
            dma((LAYERS, SIDE)), dma((LAYERS, SIDE)),
            dma((LAYERS, 2, 16)), dma((LAYERS, 2, 16)),
            dma((LAYERS,)), dma((LAYERS,)),
            dma((2, 16)), dma((2, 16)),
            dma((4,)), dma((4,)),
        ],
        compiler_params=pltpu.CompilerParams(
            collective_id=0, has_side_effects=True, vmem_limit_bytes=58 * 1024 * 1024
        ),
    )(
        residual_in, norm_gain, gate_proj, filter_proj, signal_proj, jnp.transpose(conv_taps, (1, 0, 2)), out_proj,
        final_gain.reshape(1, -1),
    )


def solution(mesh):
    return jax.shard_map(
        per_device,
        mesh=mesh,
        in_specs=(
            P("sp", "tp"),
            P(),
            P(None, "sp", "tp"),
            P(None, "sp", "tp"),
            P(None, "sp", "tp"),
            P(None, None, "tp"),
            P(None, "tp", "sp"),
            P("tp"),
        ),
        out_specs=P("sp", "tp"),
        check_vma=False,
    )
```

```python
import jax
import jax.numpy as jnp
from jax import lax
from jax.experimental import pallas as pl
from jax.experimental.pallas import tpu as pltpu
from jax.sharding import PartitionSpec as P

D = 4096
TAPS = 3
LAYERS = 2
FLOOR = 1e-06

NZ = 8
SIDE = 4
ROWS = 256
PIECE = 512
COLS = 256
CH = 128
WIDE = 512

F32 = jnp.float32
BF16 = jnp.bfloat16
MESH = pl.DeviceIdType.MESH

GATHER = (((96, 80), (176, 80), (0, 48), (48, 48)), ((112, 80), (192, 64), (0, 64), (64, 48)))
REDUCE = (((112, 80), (192, 64), (0, 64), (64, 48)), ((128, 64), (192, 64), (0, 64), (64, 64)))
GROUPS = ((0, 1), (2, 3))


SENT_ROWS = (7680, 8192, 3584, 3584, 392)


def span(units, group):
    lo = units[GROUPS[group][0]][0]
    return lo, sum(units[u][1] for u in GROUPS[group])


def aligned(index, size):
    return pl.ds(pl.multiple_of(index * size, size), size)


def has(way, far, unit):
    return not far or (unit % 2 == 0) == (way == 0)


def kernel(
    res, norm_gain, gate, filt, sig, taps, outp, final_gain, out,
    x_all, res_other, xg, w_all, w_out, acc, prod, mixed, sq, rs_out, rs_in, halo, tap_all, gain_in, gain_out,
    sums, st, fin_out, fin_in,
    loc, sent, ag0_r, ag_r, w_r, d_r, rs_r, h_r, s_r, m_r,
):
    s = lax.axis_index("sp")
    t = lax.axis_index("tp")
    z, c = t // 2, t % 2
    y, x = s // SIDE, s % SIDE
    other = 1 - c
    partner = (s, 2 * z + other)

    def at_z(k, core=None):
        return (s, ((z + k + NZ) % NZ) * 2 + (c if core is None else core))

    def at_x(k):
        return (y * SIDE + (x + k + SIDE) % SIDE, t)

    def at_y(k):
        return (((y + k + SIDE) % SIDE) * SIDE + x, t)

    halo_next = ((s + c) % 16, 2 * z + other)
    halo_far = ((s + 2 * c + 15) % 16, 2 * z + other)

    def rdma(src, dst, send, recv, device):
        return pltpu.make_async_remote_copy(
            src_ref=src, dst_ref=dst, send_sem=send, recv_sem=recv, device_id=device, device_id_type=MESH
        )

    def start(copy):
        copy.start()

    barrier = pltpu.get_barrier_semaphore()
    peers = [at_z(1), at_z(-1), at_z(1, other), at_z(-1, other), at_x(1), at_x(-1), at_y(1), at_y(-1), partner]
    for peer in peers:
        pl.semaphore_signal(barrier, inc=1, device_id=peer, device_id_type=MESH)

    own_cols = aligned(c, COLS)
    other_cols = aligned(other, COLS)
    own_rows = aligned(c, ROWS)
    other_rows = aligned(other, ROWS)

    local = []

    def place(src, dst):
        copy = pltpu.make_async_copy(src, dst, loc.at[0])
        copy.start()
        local.append(copy)

    place(res.at[own_rows, :], x_all.at[0, z, :, own_cols])
    place(res.at[other_rows, :], res_other)
    for l in range(LAYERS):
        for part, ref in enumerate((gate, filt, sig)):
            first = pl.multiple_of(c * 3 * CH + (part + 1) * CH, CH)
            place(ref.at[l], w_all.at[l, aligned(s, 256), pl.ds(first, CH)])
        for h in range(2):
            place(
                outp.at[l, :, pl.ds(h * CH, CH)],
                w_all.at[l, aligned(2 * s + h, CH), aligned(c * 7, CH)],
            )
    place(norm_gain, gain_in)
    place(taps, tap_all.at[c])
    place(final_gain, gain_out)

    with jax.named_scope("barrier"):
        pl.semaphore_wait(barrier, len(peers))
    with jax.named_scope("local"):
        for copy in local:
            copy.wait()

    def lanes(what, core):
        if what == "proj":
            return pl.ds(pl.multiple_of(core * 3 * CH + CH, CH), 3 * CH)
        if what == "out":
            return aligned(core * 7, CH)
        return aligned(core, WIDE)

    carriers = ((0, "proj", 0, 64), (0, "proj", 64, 64), (0, "out", 0, 128), (1, "both", 0, 128))

    def w_copy(carrier, group, half, axis, across, sign, fwd, sending):
        l, what, first, size = carriers[carrier]
        step = sign if fwd else 0
        along = -step if sending else -step - sign
        lo = half * 128 + first
        if fwd:
            size = size // 2
            lo += 0 if sign == 1 else size
        if axis == 0:
            yy, xx = y + across, x + along
        else:
            yy, xx = y + along, x + across
        index = ((yy + SIDE) % SIDE) * SIDE + (xx + SIDE) % SIDE
        ref = w_all.at[l, pl.ds(pl.multiple_of(index * 256 + lo, 32), size), lanes(what, c)]
        slot = group * 4 + (2 if fwd else 0) + (0 if sign == 1 else 1)
        device = at_x(sign) if axis == 0 else at_y(sign)
        return rdma(ref, ref, sent.at[0], w_r.at[carrier % 3, slot], device)

    groups = {("a", 1): (0, 0, 0, 0), ("b", 1): (5, 1, 1, 0)}
    for i, p in enumerate((0, -1, 1, 2)):
        groups["a", 2, p] = (1 + i, 0, 1, p)
        groups["b", 2, p] = (6 + i, 1, 0, p)

    def w_send(carrier, *name):
        group, half, axis, across = groups[name]
        for sign in (1, -1):
            start(w_copy(carrier, group, half, axis, across, sign, False, True))

    def w_forward(carrier, *name):
        group, half, axis, across = groups[name]
        for sign in (1, -1):
            w_copy(carrier, group, half, axis, across, sign, False, False).wait_recv()
            start(w_copy(carrier, group, half, axis, across, sign, True, True))

    def w_finish(carrier, *name):
        group, half, axis, across = groups[name]
        for sign in (1, -1):
            w_copy(carrier, group, half, axis, across, sign, True, False).wait_recv()

    parcels = ((0, "proj"), (0, "out"), (1, "both"))

    def w_parcel(parcel, k, core):
        l, what = parcels[parcel]
        ref = w_all.at[l, aligned((y + k + SIDE) % SIDE, 1024), lanes(what, core)]
        slot = (k + SIDE) % SIDE
        return rdma(ref, ref, sent.at[1], d_r.at[parcel, slot], partner)

    def w_hand(parcel, *ks):
        for k in ks:
            start(w_parcel(parcel, k, c))

    def w_taken(parcel, k):
        with jax.named_scope(f"taken#p={parcel}#k={k}"):
            w_parcel(parcel, k, other).wait_recv()

    def w_stage(carrier, stage):
        with jax.named_scope(f"w#t={carrier}#s={stage}"):
            w_stage_body(carrier, stage)

    def w_stage_body(t, stage):
        if stage == 0:
            w_send(t, "a", 1)
            w_send(t, "b", 1)
            w_send(t, "b", 2, 0)
            w_send(t, "a", 2, 0)
        elif stage == 1:
            w_forward(t, "a", 1)
            w_forward(t, "b", 1)
            for p in (-1, 1):
                w_send(t, "a", 2, p)
                w_send(t, "b", 2, p)
        elif stage == 2:
            w_forward(t, "b", 2, 0)
            w_forward(t, "a", 2, 0)
            w_finish(t, "a", 1)
            w_send(t, "a", 2, 2)
            w_finish(t, "b", 1)
            w_send(t, "b", 2, 2)
        elif stage == 3:
            for p in (-1, 1):
                w_forward(t, "a", 2, p)
                w_forward(t, "b", 2, p)
            w_finish(t, "a", 2, 0)
            w_finish(t, "b", 2, 0)
        elif stage == 4:
            w_forward(t, "a", 2, 2)
            w_forward(t, "b", 2, 2)
            for p in (-1, 1):
                w_finish(t, "a", 2, p)
                w_finish(t, "b", 2, p)
        else:
            w_finish(t, "a", 2, 2)
            w_finish(t, "b", 2, 2)

    def build_w_out(l, k):
        first = ((y + k + SIDE) % SIDE) * 8

        def body(i, carry):
            for core in range(2):
                w_out[core * CH : (core + 1) * CH, aligned(first + i, CH)] = w_all[
                    l, aligned(first + i, CH), core * 7 * CH : (core * 7 + 1) * CH
                ]
            return carry

        lax.fori_loop(0, 8, body, 0)

    def chunk_at(k):
        return (z + k + NZ) % NZ

    def ag_copy(l, way, dist, unit, sending):
        sign = 1 - 2 * way
        lo, size = GATHER[l][unit]
        ref = x_all.at[l, chunk_at(-sign * (dist if sending else dist + 1)), pl.ds(lo, size), :]
        slot = dist * 4 + unit
        return rdma(ref, ref, sent.at[2], ag_r.at[way, slot], at_z(sign))

    def first_copy(way, unit, crossing, sending):
        sign = 1 - 2 * way
        lo, size = GATHER[0][unit]
        cols = own_cols if sending or not crossing else other_cols
        dst = x_all.at[0, z if sending else chunk_at(-sign), pl.ds(lo, size), cols]
        src = res_other.at[pl.ds(lo, size), :] if crossing else x_all.at[0, z, pl.ds(lo, size), own_cols]
        slot = unit * 2 + (1 if crossing else 0)
        return rdma(src, dst, sent.at[2], ag0_r.at[way, slot], at_z(sign, other if crossing else c))

    def ag_first(l, unit):
        for way in range(2):
            if l == 0:
                start(first_copy(way, unit, False, True))
                start(first_copy(way, unit, True, True))
            else:
                start(ag_copy(l, way, 0, unit, True))

    def ag_step(l, dist, unit):
        with jax.named_scope(f"ag#l={l}#d={dist}#u={unit}"):
            for way in range(2):
                if not has(way, dist == 3, unit):
                    continue
                if l == 0 and dist == 0:
                    first_copy(way, unit, False, False).wait_recv()
                    first_copy(way, unit, True, False).wait_recv()
                else:
                    ag_copy(l, way, dist, unit, False).wait_recv()
                if dist < 3 and has(way, dist == 2, unit):
                    start(ag_copy(l, way, dist + 1, unit, True))

    def take(l, group, chunk):
        lo, size = span(GATHER[l], group)
        rows = pl.ds(lo, size)
        value = x_all[l, chunk, rows, :].astype(F32)
        square = value * value
        total = square[:, :128]
        for i in range(1, PIECE // 128):
            total = total + square[:, i * 128 : (i + 1) * 128]
        sq[rows, :] += total
        xg[chunk, rows, :] = (value * gain_in[l : l + 1, aligned(chunk, PIECE)]).astype(BF16)

    def arrived_at(dist):
        return (-dist - 1, dist + 1) if dist < 3 else (4,)

    def multiply(l, group, chunk):
        lo, size = span(GATHER[l], group)
        acc[lo : lo + size, :] += jnp.dot(
            xg[chunk, lo : lo + size, :],
            w_all[l, aligned(chunk, PIECE), CH : 7 * CH],
            preferred_element_type=F32,
        )

    def multiply_row(l, group, k):
        first = ((y + k + SIDE) % SIDE) * 2
        with jax.named_scope(f"mult#g={group}"):
            multiply(l, group, first)
            multiply(l, group, first + 1)

    def start_sums():
        sq[...] = jnp.zeros_like(sq)
        acc[...] = jnp.zeros_like(acc)

    def gates(l, group):
        lo, size = span(GATHER[l], group)
        rows = pl.ds(lo, size)
        mean = jnp.sum(sq[rows, :], axis=1, keepdims=True) / D
        scale = lax.rsqrt(mean + FLOOR)
        for core in range(2):
            base = core * 3 * CH
            value = (acc[rows, base + CH : base + 2 * CH] * scale) * (acc[rows, base + 2 * CH : base + 3 * CH] * scale)
            prod[pl.ds(8 + lo, size), core * CH : (core + 1) * CH] = value.astype(BF16).astype(F32)
            acc[rows, base : base + CH] = acc[rows, base : base + CH] * scale

    def mix(l, unit):
        lo, size = REDUCE[l][unit]
        rows = pl.ds(lo, size)
        for core in range(2):
            cols = pl.ds(core * CH, CH)
            filtered = jnp.zeros((size, CH), F32)
            for k in range(TAPS):
                tap = tap_all[core, k, l : l + 1, :]
                filtered = filtered + tap * prod[pl.ds(8 + lo - (TAPS - 1) + k, size), cols]
            gated = acc[rows, core * 3 * CH : core * 3 * CH + CH]
            mixed[rows, cols] = (gated * filtered).astype(BF16)

    def halo_copy(l):
        return rdma(halo.at[l, 0], halo.at[l, 1], sent.at[4], h_r.at[l], halo_next)

    def give_halo(l):
        halo[l, 0] = prod[ROWS:, :]
        start(halo_copy(l))

    def take_halo(l):
        with jax.named_scope("halo"):
            halo_copy(l).wait_recv()
        first = jnp.logical_and(s == 0, c == 0)
        prod[:8, :] = jnp.where(first, 0.0, halo[l, 1])

    def rs_copy(l, way, k, unit):
        lo, size = REDUCE[l][unit]
        rows = pl.ds(lo, size)
        slot = (k - 1) * 4 + unit
        return rdma(
            rs_out.at[l, way, k - 1, rows, :], rs_in.at[l, way, k - 1, rows, :],
            sent.at[3], rs_r.at[way, slot], at_z(1 - 2 * way),
        )

    def partial(l, unit, chunk):
        lo, size = REDUCE[l][unit]
        return jnp.dot(mixed[lo : lo + size, :], w_out[:, aligned(chunk, PIECE)], preferred_element_type=F32)

    def arrived(l, way, k, unit):
        rs_copy(l, way, k, unit).wait_recv()
        lo, size = REDUCE[l][unit]
        return rs_in[l, way, k - 1, lo : lo + size, :].astype(F32)

    def rs_step(l, i, unit):
        with jax.named_scope(f"rs#l={l}#i={i}#u={unit}"):
            lo, size = REDUCE[l][unit]
            for way in range(2):
                k = 4 - i if has(way, True, unit) else 3 - i
                if k < 1:
                    continue
                value = partial(l, unit, chunk_at(k * (1 - 2 * way)))
                if i > 0:
                    value = value + arrived(l, way, k + 1, unit)
                rs_out[l, way, k - 1, lo : lo + size, :] = value.astype(BF16)
                start(rs_copy(l, way, k, unit))

    def rs_last(l, unit):
        with jax.named_scope(f"last#l={l}#u={unit}"):
            lo, size = REDUCE[l][unit]
            value = partial(l, unit, z)
            for way in range(2):
                value = value + arrived(l, way, 1, unit)
            return (x_all[l, z, lo : lo + size, :].astype(F32) + value).astype(BF16)

    def take_step(l, group, dist):
        for k in arrived_at(dist):
            take(l, group, chunk_at(k))
            if l == 1:
                multiply(l, group, chunk_at(k))

    ag_first(0, 0)
    ag_first(0, 1)
    w_stage(0, 0)
    w_stage(1, 0)
    start(rdma(res_other, x_all.at[0, z, :, own_cols], sent.at[4], m_r.at[0], partner))
    start(rdma(tap_all.at[c], tap_all.at[c], sent.at[5], m_r.at[1], partner))
    ag_first(0, 2)
    ag_first(0, 3)
    start_sums()
    rdma(res_other, x_all.at[0, z, :, other_cols], sent.at[4], m_r.at[0], partner).wait_recv()
    take(0, 0, z)
    take(0, 1, z)

    w_stage(2, 0)
    w_stage(0, 1)
    ag_step(0, 0, 0)
    w_stage(1, 1)
    ag_step(0, 0, 1)
    take_step(0, 0, 0)
    ag_step(0, 0, 2)
    ag_step(0, 0, 3)
    take_step(0, 1, 0)
    w_stage(2, 1)
    w_stage(0, 2)
    ag_step(0, 1, 0)
    w_stage(1, 2)
    ag_step(0, 1, 1)
    take_step(0, 0, 1)
    ag_step(0, 1, 2)
    w_stage(0, 3)
    ag_step(0, 1, 3)
    take_step(0, 1, 1)
    w_stage(2, 2)
    w_stage(1, 3)
    w_hand(0, 0)
    ag_step(0, 2, 0)
    w_stage(0, 4)
    ag_step(0, 2, 1)
    take_step(0, 0, 2)
    w_stage(2, 3)
    w_stage(1, 4)
    w_hand(0, -1, 1)
    w_hand(1, 0)
    ag_step(0, 2, 2)
    ag_step(0, 2, 3)
    take_step(0, 1, 2)
    w_stage(0, 5)
    w_stage(2, 4)
    w_hand(1, -1, 1)
    ag_step(0, 3, 0)
    ag_step(0, 3, 1)
    take_step(0, 0, 3)
    w_stage(1, 5)
    w_hand(0, 2)
    w_taken(0, 0)
    multiply_row(0, 0, 0)
    w_taken(0, -1)
    multiply_row(0, 0, -1)
    w_stage(2, 5)
    w_hand(1, 2)
    w_stage(3, 0)
    for k in (1, 2):
        w_taken(0, k)
        multiply_row(0, 0, k)
    ag_step(0, 3, 2)
    ag_step(0, 3, 3)
    take_step(0, 1, 3)
    gates(0, 0)
    rdma(tap_all.at[other], tap_all.at[other], sent.at[4], m_r.at[1], partner).wait_recv()
    give_halo(0)
    mix(0, 1)
    mix(0, 0)
    for k in (0, -1, 1, 2):
        w_taken(1, k)
        build_w_out(0, k)

    rs_step(0, 0, 1)
    rs_step(0, 0, 0)
    for k in (0, -1, 1, 2):
        multiply_row(0, 1, k)
    gates(0, 1)
    mix(0, 3)
    rs_step(0, 0, 3)
    rs_step(0, 1, 1)
    take_halo(0)
    mix(0, 2)
    rs_step(0, 0, 2)
    start_sums()
    rs_step(0, 1, 0)
    rs_step(0, 1, 3)
    w_stage(3, 1)
    rs_step(0, 2, 1)
    rs_step(0, 1, 2)
    rs_step(0, 2, 0)
    rs_step(0, 2, 3)
    w_stage(3, 2)
    rs_step(0, 3, 1)
    rs_step(0, 2, 2)
    rs_step(0, 3, 0)
    rs_step(0, 3, 3)
    w_stage(3, 3)
    w_hand(2, 0)

    def next_stream(unit):
        lo, size = REDUCE[0][unit]
        x_all[1, z, lo : lo + size, :] = rs_last(0, unit)
        ag_first(1, unit)

    next_stream(1)
    rs_step(0, 3, 2)
    next_stream(0)
    take(1, 0, z)
    next_stream(3)
    next_stream(2)
    take(1, 1, z)

    ag_step(1, 0, 1)
    ag_step(1, 0, 0)
    w_stage(3, 4)
    w_hand(2, -1, 1)
    ag_step(1, 0, 3)
    ag_step(1, 0, 2)
    ag_step(1, 1, 1)
    ag_step(1, 1, 0)
    w_stage(3, 5)
    w_hand(2, 2)
    ag_step(1, 1, 3)
    ag_step(1, 1, 2)
    for k in (0, -1, 1, 2):
        w_taken(2, k)
        build_w_out(1, k)
    ag_step(1, 2, 1)
    for group in range(2):
        multiply(1, group, z)
        take_step(1, group, 0)
    ag_step(1, 2, 0)
    take_step(1, 0, 1)
    ag_step(1, 2, 3)
    take_step(1, 1, 1)
    ag_step(1, 2, 2)
    take_step(1, 0, 2)
    take_step(1, 1, 2)
    ag_step(1, 3, 1)
    ag_step(1, 3, 0)
    take_step(1, 0, 3)
    gates(1, 0)
    give_halo(1)
    mix(1, 1)
    mix(1, 0)
    rs_step(1, 0, 1)
    rs_step(1, 0, 0)
    ag_step(1, 3, 3)
    ag_step(1, 3, 2)
    take_step(1, 1, 3)
    gates(1, 1)
    mix(1, 3)
    rs_step(1, 0, 3)
    rs_step(1, 1, 1)
    take_halo(1)
    mix(1, 2)
    rs_step(1, 0, 2)
    rs_step(1, 1, 0)
    rs_step(1, 1, 3)
    rs_step(1, 2, 1)
    rs_step(1, 1, 2)
    rs_step(1, 2, 0)
    rs_step(1, 2, 3)
    rs_step(1, 3, 1)
    rs_step(1, 2, 2)
    rs_step(1, 3, 0)
    rs_step(1, 3, 3)
    rs_step(1, 3, 2)

    def fin_copy(group):
        rows = pl.ds(*span(REDUCE[1], group))
        return rdma(fin_out.at[rows, :], fin_in.at[rows, :], sent.at[4], m_r.at[2 + group], partner)

    def sums_copy(group, k, crossing):
        ref = sums.at[c, z, :, pl.ds(*span(REDUCE[1], group))]
        return rdma(ref, ref, sent.at[4], s_r.at[group, crossing], at_z(k, other if crossing else c))

    routes = [(4, 0), (4, 1), (3, 0), (3, 1), (5, 0), (5, 1), (2, 0), (2, 1), (6, 0), (6, 1)]
    routes += [(1, 0), (1, 1), (7, 0), (7, 1), (0, 1)]
    for group in range(2):
        for unit in GROUPS[group]:
            lo, size = REDUCE[1][unit]
            st[lo : lo + size, :] = rs_last(1, unit).astype(F32)
        lo, size = span(REDUCE[1], group)
        rows = pl.ds(lo, size)
        value = st[rows, :]
        square = jnp.sum(value * value, axis=1, keepdims=True)
        sums[c, z, :, lo : lo + size] = jnp.broadcast_to(square, (size, 128)).T[:8, :]
        for k, crossing in routes:
            start(sums_copy(group, k, crossing))
        fin_out[rows, :] = st[rows, other_cols].astype(BF16)
        start(fin_copy(group))

    def scale_of(core):
        total = jnp.sum(sums[core, :, 0, :], axis=0, keepdims=True)
        return lax.rsqrt(jnp.broadcast_to(total, (128, ROWS)).T[:, :1] / D + FLOOR)

    with jax.named_scope("sums"):
        for group in range(2):
            fin_copy(group).wait_recv()
            cols = pl.ds(*span(REDUCE[1], group))
            for crossing, ref in enumerate((sums.at[c, pl.ds(0, NZ - 1), :, cols], sums.at[other, :, :, cols])):
                rdma(ref, ref, sent.at[4], s_r.at[group, crossing], partner).wait_recv()
    out[own_rows, :] = st[:, own_cols] * scale_of(c) * gain_out[...]
    out[other_rows, :] = fin_in[...].astype(F32) * scale_of(other) * gain_out[...]
    with jax.named_scope("sends"):
        for kind, rows in enumerate(SENT_ROWS):
            ref = w_all.at[0, pl.ds(0, rows), pl.ds(0, WIDE)] if rows <= D else w_all.at[0, pl.ds(0, rows // 2), :]
            rdma(ref, ref, sent.at[kind], m_r.at[0], partner).wait_send()
        rdma(tap_all.at[c], tap_all.at[c], sent.at[5], m_r.at[1], partner).wait_send()


def per_device(residual_in, norm_gain, gate_proj, filter_proj, signal_proj, conv_taps, out_proj, final_gain):
    dma = pltpu.SemaphoreType.DMA
    return pl.pallas_call(
        kernel,
        out_shape=jax.ShapeDtypeStruct((2 * ROWS, COLS), F32),
        in_specs=[pl.BlockSpec(memory_space=pltpu.HBM)] * 8,
        out_specs=pl.BlockSpec(memory_space=pltpu.VMEM),
        scratch_shapes=[
            pltpu.VMEM((LAYERS, NZ, ROWS, PIECE), BF16),
            pltpu.VMEM((ROWS, COLS), BF16),
            pltpu.VMEM((NZ, ROWS, PIECE), BF16),
            pltpu.VMEM((LAYERS, D, 2 * WIDE), BF16),
            pltpu.VMEM((2 * CH, D), BF16),
            pltpu.VMEM((ROWS, 6 * CH), F32),
            pltpu.VMEM((8 + ROWS, 2 * CH), F32),
            pltpu.VMEM((ROWS, 2 * CH), BF16),
            pltpu.VMEM((ROWS, 128), F32),
            pltpu.VMEM((LAYERS, 2, 4, ROWS, PIECE), BF16),
            pltpu.VMEM((LAYERS, 2, 4, ROWS, PIECE), BF16),
            pltpu.VMEM((LAYERS, 2, 8, 2 * CH), F32),
            pltpu.VMEM((2, TAPS, LAYERS, CH), F32),
            pltpu.VMEM((LAYERS, D), F32),
            pltpu.VMEM((1, COLS), F32),
            pltpu.VMEM((2, NZ, 8, ROWS), F32),
            pltpu.VMEM((ROWS, PIECE), F32),
            pltpu.VMEM((ROWS, COLS), BF16),
            pltpu.VMEM((ROWS, COLS), BF16),
            dma((1,)),
            dma((6,)),
            dma((2, 8)),
            dma((2, 16)),
            dma((3, 40)),
            dma((3, SIDE)),
            dma((2, 16)),
            dma((LAYERS,)),
            dma((2, 2)),
            dma((4,)),
        ],
        compiler_params=pltpu.CompilerParams(
            collective_id=0, has_side_effects=True, vmem_limit_bytes=44 * 1024 * 1024
        ),
    )(
        *(
            pltpu.with_memory_space_constraint(a, pltpu.HBM)
            for a in (
                residual_in, norm_gain, gate_proj, filter_proj, signal_proj, jnp.transpose(conv_taps, (1, 0, 2)),
                out_proj, final_gain.reshape(1, -1),
            )
        )
    )


def solution(mesh):
    return jax.shard_map(
        per_device,
        mesh=mesh,
        in_specs=(
            P("sp", "tp"),
            P(),
            P(None, "sp", "tp"),
            P(None, "sp", "tp"),
            P(None, "sp", "tp"),
            P(None, None, "tp"),
            P(None, "tp", "sp"),
            P("tp"),
        ),
        out_specs=P("sp", "tp"),
        check_vma=False,
    )
```

```python
import jax
import jax.numpy as jnp
from jax import lax
from jax.experimental import pallas as pl
from jax.experimental.pallas import tpu as pltpu
from jax.sharding import PartitionSpec as P

D = 4096
TAPS = 3
LAYERS = 2
FLOOR = 1e-06

NZ = 8
SIDE = 4
ROWS = 256
PIECE = 512
COLS = 256
CH = 128
WIDE = 512

F32 = jnp.float32
BF16 = jnp.bfloat16
MESH = pl.DeviceIdType.MESH

GATHER = (
    ((96, 80), (176, 80), (0, 16), (16, 48), (64, 32)),
    ((112, 80), (192, 64), (0, 16), (16, 48), (64, 48)),
)
REDUCE = (
    ((112, 80), (192, 64), (0, 16), (16, 48), (64, 48)),
    ((128, 64), (192, 64), (0, 16), (16, 64), (80, 48)),
)
GROUPS = ((0, 1), (2, 3, 4))
UNITS = 5
FAR = (0, 1, 1, 0, 1)

SENT_ROWS = (7680, 8192, 3584, 3584, 392)


def span(units, group):
    lo = units[GROUPS[group][0]][0]
    return lo, sum(units[u][1] for u in GROUPS[group])


def aligned(index, size):
    return pl.ds(pl.multiple_of(index * size, size), size)


def has(way, far, unit):
    return not far or FAR[unit] == way


def kernel(
    res, norm_gain, gate, filt, sig, taps, outp, final_gain, out,
    x_all, res_other, xg, w_all, w_out, acc, prod, mixed, sq, rs_out, rs_in, halo, tap_all, gain_in, gain_out,
    sums, st, fin_out, fin_in,
    loc, sent, ag_r, w_r, d_r, rs_r, h_r, s_r, m_r,
):
    s = lax.axis_index("sp")
    t = lax.axis_index("tp")
    z, c = t // 2, t % 2
    y, x = s // SIDE, s % SIDE
    other = 1 - c
    partner = (s, 2 * z + other)

    def at_z(k, core=None):
        return (s, ((z + k + NZ) % NZ) * 2 + (c if core is None else core))

    def at_x(k):
        return (y * SIDE + (x + k + SIDE) % SIDE, t)

    def at_y(k):
        return (((y + k + SIDE) % SIDE) * SIDE + x, t)

    half = 1 - c
    halo_next = ((s + half) % 16, 2 * z + other)

    def rdma(src, dst, send, recv, device):
        return pltpu.make_async_remote_copy(
            src_ref=src, dst_ref=dst, send_sem=send, recv_sem=recv, device_id=device, device_id_type=MESH
        )

    def start(copy):
        copy.start()

    barrier = pltpu.get_barrier_semaphore()
    peers = [at_z(1), at_z(-1), at_z(1, other), at_z(-1, other), at_x(1), at_x(-1), at_y(1), at_y(-1), partner]
    for peer in peers:
        pl.semaphore_signal(barrier, inc=1, device_id=peer, device_id_type=MESH)

    own_cols = aligned(c, COLS)
    other_cols = aligned(other, COLS)
    own_rows = aligned(half, ROWS)
    other_rows = aligned(1 - half, ROWS)

    local = []

    def place(src, dst):
        copy = pltpu.make_async_copy(src, dst, loc.at[0])
        copy.start()
        local.append(copy)

    place(res.at[own_rows, :], x_all.at[0, z, :, own_cols])
    place(res.at[other_rows, :], res_other)
    for l in range(LAYERS):
        for part, ref in enumerate((gate, filt, sig)):
            first = pl.multiple_of(c * 3 * CH + (part + 1) * CH, CH)
            place(ref.at[l], w_all.at[l, aligned(s, 256), pl.ds(first, CH)])
        for h in range(2):
            place(
                outp.at[l, :, pl.ds(h * CH, CH)],
                w_all.at[l, aligned(2 * s + h, CH), aligned(c * 7, CH)],
            )
    place(norm_gain, gain_in)
    place(taps, tap_all.at[c])
    place(final_gain, gain_out)

    with jax.named_scope("barrier"):
        pl.semaphore_wait(barrier, len(peers))
    with jax.named_scope("local"):
        for copy in local:
            copy.wait()

    def lanes(what, core):
        if what == "proj":
            return pl.ds(pl.multiple_of(core * 3 * CH + CH, CH), 3 * CH)
        if what == "out":
            return aligned(core * 7, CH)
        return aligned(core, WIDE)

    carriers = ((0, "proj", 0, 64), (0, "proj", 64, 64), (0, "out", 0, 128), (1, "both", 0, 128))

    def w_copy(carrier, group, half, axis, across, sign, fwd, sending):
        l, what, first, size = carriers[carrier]
        step = sign if fwd else 0
        along = -step if sending else -step - sign
        lo = half * 128 + first
        if fwd:
            size = size // 2
            lo += 0 if sign == 1 else size
        if axis == 0:
            yy, xx = y + across, x + along
        else:
            yy, xx = y + along, x + across
        index = ((yy + SIDE) % SIDE) * SIDE + (xx + SIDE) % SIDE
        ref = w_all.at[l, pl.ds(pl.multiple_of(index * 256 + lo, 32), size), lanes(what, c)]
        slot = group * 2 + (1 if fwd else 0)
        device = at_x(sign) if axis == 0 else at_y(sign)
        return rdma(ref, ref, sent.at[0], w_r.at[carrier % 3, slot], device)

    groups = {("a", 1): (0, 0, 0, 0), ("b", 1): (5, 1, 1, 0)}
    for i, p in enumerate((0, -1, 1, 2)):
        groups["a", 2, p] = (1 + i, 0, 1, p)
        groups["b", 2, p] = (6 + i, 1, 0, p)

    def w_send(carrier, *name):
        group, half, axis, across = groups[name]
        for sign in (1, -1):
            start(w_copy(carrier, group, half, axis, across, sign, False, True))

    def w_wait(carrier, group, fwd):
        l, what, _, size = carriers[carrier]
        ref = w_all.at[l, pl.ds(0, size if fwd else 2 * size), lanes(what, c)]
        rdma(ref, ref, sent.at[0], w_r.at[carrier % 3, group * 2 + (1 if fwd else 0)], partner).wait_recv()

    def w_forward(carrier, *name):
        group, half, axis, across = groups[name]
        w_wait(carrier, group, False)
        for sign in (1, -1):
            start(w_copy(carrier, group, half, axis, across, sign, True, True))

    def w_finish(carrier, *name):
        w_wait(carrier, groups[name][0], True)

    parcels = ((0, "proj"), (0, "out"), (1, "both"))

    def w_parcel(parcel, k, core):
        l, what = parcels[parcel]
        ref = w_all.at[l, aligned((y + k + SIDE) % SIDE, 1024), lanes(what, core)]
        slot = (k + SIDE) % SIDE
        return rdma(ref, ref, sent.at[1], d_r.at[parcel, slot], partner)

    def w_hand(parcel, *ks):
        for k in ks:
            start(w_parcel(parcel, k, c))

    def w_taken(parcel, k):
        with jax.named_scope(f"taken#p={parcel}#k={k}"):
            w_parcel(parcel, k, other).wait_recv()

    def w_stage(carrier, stage):
        with jax.named_scope(f"w#t={carrier}#s={stage}"):
            w_stage_body(carrier, stage)

    def w_stage_body(t, stage):
        if stage == 0:
            w_send(t, "a", 1)
            w_send(t, "b", 1)
            w_send(t, "b", 2, 0)
            w_send(t, "a", 2, 0)
        elif stage == 1:
            w_forward(t, "a", 1)
            w_forward(t, "b", 1)
            for p in (-1, 1):
                w_send(t, "a", 2, p)
                w_send(t, "b", 2, p)
            w_forward(t, "b", 2, 0)
            w_forward(t, "a", 2, 0)
        elif stage == 2:
            w_finish(t, "a", 1)
            w_send(t, "a", 2, 2)
            w_finish(t, "b", 1)
            w_send(t, "b", 2, 2)
        elif stage == 3:
            for p in (-1, 1):
                w_forward(t, "a", 2, p)
                w_forward(t, "b", 2, p)
        else:
            w_forward(t, "a", 2, 2)
            w_forward(t, "b", 2, 2)

    def w_end(parcel, *ks):
        with jax.named_scope(f"end#p={parcel}#k={ks[0]}"):
            for k in ks:
                for t in ((0, 1), (2,), (3,))[parcel]:
                    w_finish(t, "a", 2, k)
                    w_finish(t, "b", 2, k)
        w_hand(parcel, *ks)

    def build_w_out(l, k):
        first = ((y + k + SIDE) % SIDE) * 8

        def body(i, carry):
            for core in range(2):
                w_out[core * CH : (core + 1) * CH, aligned(first + i, CH)] = w_all[
                    l, aligned(first + i, CH), core * 7 * CH : (core * 7 + 1) * CH
                ]
            return carry

        lax.fori_loop(0, 8, body, 0)

    def chunk_at(k):
        return (z + k + NZ) % NZ

    def ag_copy(l, way, dist, unit):
        sign = 1 - 2 * way
        lo, size = GATHER[l][unit]
        ref = x_all.at[l, chunk_at(-sign * dist), pl.ds(lo, size), :]
        return rdma(ref, ref, sent.at[2], ag_r.at[dist * UNITS + unit], at_z(sign))

    def first_copy(way, unit, crossing):
        lo, size = GATHER[0][unit]
        dst = x_all.at[0, z, pl.ds(lo, size), own_cols]
        src = res_other.at[pl.ds(lo, size), :] if crossing else dst
        return rdma(src, dst, sent.at[2], ag_r.at[unit], at_z(1 - 2 * way, other if crossing else c))

    def ag_first(l, unit):
        for way in range(2):
            if l == 0:
                start(first_copy(way, unit, False))
                start(first_copy(way, unit, True))
            else:
                start(ag_copy(l, way, 0, unit))

    def ag_step(l, dist, unit):
        with jax.named_scope(f"ag#l={l}#d={dist}#u={unit}"):
            _, size = GATHER[l][unit]
            ref = x_all.at[l, 0, pl.ds(0, size if dist == 3 else 2 * size), :]
            rdma(ref, ref, sent.at[2], ag_r.at[dist * UNITS + unit], partner).wait_recv()
            for way in range(2):
                if dist < 3 and has(way, dist == 2, unit):
                    start(ag_copy(l, way, dist + 1, unit))

    def take(l, group, chunk):
        take_rows(l, span(GATHER[l], group), chunk)

    def take_rows(l, which, chunk):
        lo, size = which
        rows = pl.ds(lo, size)
        value = x_all[l, chunk, rows, :].astype(F32)
        square = value * value
        total = square[:, :128]
        for i in range(1, PIECE // 128):
            total = total + square[:, i * 128 : (i + 1) * 128]
        sq[rows, :] += total
        xg[chunk, rows, :] = (value * gain_in[l : l + 1, aligned(chunk, PIECE)]).astype(BF16)

    def arrived_at(dist):
        return (-dist - 1, dist + 1) if dist < 3 else (4,)

    def multiply(l, group, chunk):
        multiply_rows(l, span(GATHER[l], group), chunk)

    def multiply_rows(l, which, chunk):
        lo, size = which
        acc[lo : lo + size, :] += jnp.dot(
            xg[chunk, lo : lo + size, :],
            w_all[l, aligned(chunk, PIECE), CH : 7 * CH],
            preferred_element_type=F32,
        )

    def multiply_row(l, group, k):
        first = ((y + k + SIDE) % SIDE) * 2
        with jax.named_scope(f"mult#g={group}"):
            multiply(l, group, first)
            multiply(l, group, first + 1)

    def start_sums():
        sq[...] = jnp.zeros_like(sq)
        acc[...] = jnp.zeros_like(acc)

    def gates(l, group):
        gates_rows(l, span(GATHER[l], group))

    def gates_rows(l, which):
        lo, size = which
        rows = pl.ds(lo, size)
        mean = jnp.sum(sq[rows, :], axis=1, keepdims=True) / D
        scale = lax.rsqrt(mean + FLOOR)
        for core in range(2):
            base = core * 3 * CH
            value = (acc[rows, base + CH : base + 2 * CH] * scale) * (acc[rows, base + 2 * CH : base + 3 * CH] * scale)
            prod[pl.ds(8 + lo, size), core * CH : (core + 1) * CH] = value.astype(BF16).astype(F32)
            acc[rows, base : base + CH] = acc[rows, base : base + CH] * scale

    def mix(l, unit):
        lo, size = REDUCE[l][unit]
        rows = pl.ds(lo, size)
        for core in range(2):
            cols = pl.ds(core * CH, CH)
            filtered = jnp.zeros((size, CH), F32)
            for k in range(TAPS):
                tap = tap_all[core, k, l : l + 1, :]
                filtered = filtered + tap * prod[pl.ds(8 + lo - (TAPS - 1) + k, size), cols]
            gated = acc[rows, core * 3 * CH : core * 3 * CH + CH]
            mixed[rows, cols] = (gated * filtered).astype(BF16)

    def halo_copy(l):
        return rdma(halo.at[l, 0], halo.at[l, 1], sent.at[4], h_r.at[l], halo_next)

    def give_halo(l):
        halo[l, 0] = prod[ROWS:, :]
        start(halo_copy(l))

    def take_halo(l):
        with jax.named_scope("halo"):
            halo_copy(l).wait_recv()
        first = jnp.logical_and(s == 0, half == 0)
        prod[:8, :] = jnp.where(first, 0.0, halo[l, 1])

    def rs_copy(l, i, way, k, unit):
        lo, size = REDUCE[l][unit]
        rows = pl.ds(lo, size)
        return rdma(
            rs_out.at[l, way, k - 1, rows, :], rs_in.at[l, way, k - 1, rows, :],
            sent.at[3], rs_r.at[i * UNITS + unit], at_z(1 - 2 * way),
        )

    def partial(l, unit, chunk):
        lo, size = REDUCE[l][unit]
        return jnp.dot(mixed[lo : lo + size, :], w_out[:, aligned(chunk, PIECE)], preferred_element_type=F32)

    def rs_wait(l, i, unit):
        _, size = REDUCE[l][unit]
        ref = rs_in.at[l, 0, 0, pl.ds(0, size if i == 3 else 2 * size), :]
        rdma(ref, ref, sent.at[3], rs_r.at[i * UNITS + unit], partner).wait_recv()

    def arrived(l, way, k, unit):
        lo, size = REDUCE[l][unit]
        return rs_in[l, way, k - 1, lo : lo + size, :].astype(F32)

    def rs_step(l, i, unit):
        with jax.named_scope(f"rs#l={l}#i={i}#u={unit}"):
            lo, size = REDUCE[l][unit]
            if i > 0:
                rs_wait(l, i - 1, unit)
            for way in range(2):
                k = 4 - i if has(way, True, unit) else 3 - i
                if k < 1:
                    continue
                value = partial(l, unit, chunk_at(k * (1 - 2 * way)))
                if i > 0:
                    value = value + arrived(l, way, k + 1, unit)
                rs_out[l, way, k - 1, lo : lo + size, :] = value.astype(BF16)
                start(rs_copy(l, i, way, k, unit))

    def rs_last(l, unit):
        with jax.named_scope(f"last#l={l}#u={unit}"):
            lo, size = REDUCE[l][unit]
            value = partial(l, unit, z)
            rs_wait(l, 3, unit)
            for way in range(2):
                value = value + arrived(l, way, 1, unit)
            return (x_all[l, z, lo : lo + size, :].astype(F32) + value).astype(BF16)

    def take_step(l, group, dist):
        for k in arrived_at(dist):
            take(l, group, chunk_at(k))
            if l == 1:
                multiply(l, group, chunk_at(k))

    ag_first(0, 0)
    ag_first(0, 1)
    w_stage(0, 0)
    w_stage(1, 0)
    start(rdma(res_other, x_all.at[0, z, :, own_cols], sent.at[4], m_r.at[0], partner))
    start(rdma(tap_all.at[c], tap_all.at[c], sent.at[5], m_r.at[1], partner))
    for unit in (3, 4, 2):
        ag_first(0, unit)
    start_sums()
    rdma(res_other, x_all.at[0, z, :, other_cols], sent.at[4], m_r.at[0], partner).wait_recv()
    take(0, 0, z)
    take(0, 1, z)

    w_stage(2, 0)
    w_stage(0, 1)
    ag_step(0, 0, 0)
    w_stage(1, 1)
    ag_step(0, 0, 1)
    take_step(0, 0, 0)
    ag_step(0, 0, 3)
    ag_step(0, 0, 4)
    w_stage(0, 2)
    ag_step(0, 0, 2)
    take_step(0, 1, 0)
    w_stage(2, 1)
    w_stage(1, 2)
    ag_step(0, 1, 0)
    w_stage(0, 3)
    ag_step(0, 1, 1)
    take_step(0, 0, 1)
    w_stage(2, 2)
    w_stage(1, 3)
    ag_step(0, 1, 3)
    ag_step(0, 1, 4)
    w_stage(0, 4)
    ag_step(0, 1, 2)
    take_step(0, 1, 1)
    w_stage(1, 4)
    w_stage(2, 3)
    w_end(0, 0)
    ag_step(0, 2, 0)
    w_stage(2, 4)
    ag_step(0, 2, 1)
    take_step(0, 0, 2)
    w_end(0, -1, 1)
    w_end(1, 0)
    ag_step(0, 2, 3)
    ag_step(0, 2, 4)
    w_end(0, 2)
    ag_step(0, 2, 2)
    take_step(0, 1, 2)
    w_end(1, -1, 1)
    ag_step(0, 3, 0)
    ag_step(0, 3, 1)
    take_step(0, 0, 3)
    w_end(1, 2)
    w_stage(3, 0)
    for k in (0, -1, 1, 2):
        w_taken(0, k)
        multiply_row(0, 0, k)
    for unit in (3, 4, 2):
        ag_step(0, 3, unit)
    take_step(0, 1, 3)
    gates(0, 0)
    rdma(tap_all.at[other], tap_all.at[other], sent.at[4], m_r.at[1], partner).wait_recv()
    give_halo(0)
    mix(0, 1)
    mix(0, 0)
    for k in (0, -1, 1, 2):
        w_taken(1, k)
        build_w_out(0, k)

    rs_step(0, 0, 0)
    rs_step(0, 0, 1)
    for k in (0, -1, 1, 2):
        multiply_row(0, 1, k)
    gates(0, 1)
    for unit in (3, 4):
        mix(0, unit)
        rs_step(0, 0, unit)
    rs_step(0, 1, 0)
    take_halo(0)
    mix(0, 2)
    rs_step(0, 0, 2)
    start_sums()
    for unit in (1, 3, 4):
        rs_step(0, 1, unit)
    w_stage(3, 1)
    rs_step(0, 2, 0)
    rs_step(0, 1, 2)
    for unit in (1, 3, 4):
        rs_step(0, 2, unit)
    rs_step(0, 3, 0)
    rs_step(0, 2, 2)
    w_stage(3, 2)
    for unit in (1, 3, 4):
        rs_step(0, 3, unit)

    def next_stream(unit):
        lo, size = REDUCE[0][unit]
        x_all[1, z, lo : lo + size, :] = rs_last(0, unit)
        ag_first(1, unit)

    next_stream(0)
    rs_step(0, 3, 2)
    w_stage(3, 3)
    next_stream(1)
    take(1, 0, z)
    next_stream(3)
    next_stream(4)

    ag_step(1, 0, 0)
    w_stage(3, 4)
    next_stream(2)
    take(1, 1, z)
    ag_step(1, 0, 1)
    ag_step(1, 0, 3)
    w_end(2, 0)
    w_end(2, -1, 1)
    ag_step(1, 0, 4)
    ag_step(1, 0, 2)
    ag_step(1, 1, 0)
    ag_step(1, 1, 1)
    w_end(2, 2)
    for unit in (3, 4, 2):
        ag_step(1, 1, unit)
    for k in (0, -1, 1, 2):
        w_taken(2, k)
        build_w_out(1, k)
    ag_step(1, 2, 0)
    for group in range(2):
        multiply(1, group, z)
        take_step(1, group, 0)
    ag_step(1, 2, 1)
    take_step(1, 0, 1)
    ag_step(1, 2, 3)
    take_step(1, 1, 1)
    ag_step(1, 2, 4)
    ag_step(1, 2, 2)
    take_step(1, 0, 2)
    take_step(1, 1, 2)
    for unit in (0, 1):
        ag_step(1, 3, unit)
        take_rows(1, GATHER[1][unit], chunk_at(4))
        multiply_rows(1, GATHER[1][unit], chunk_at(4))
        gates_rows(1, GATHER[1][unit])
        if unit == 1:
            give_halo(1)
        mix(1, unit)
        rs_step(1, 0, unit)
    for unit in (3, 4, 2):
        ag_step(1, 3, unit)
    take_step(1, 1, 3)
    gates(1, 1)
    for unit in (3, 4):
        mix(1, unit)
        rs_step(1, 0, unit)
    rs_step(1, 1, 0)
    take_halo(1)
    mix(1, 2)
    rs_step(1, 0, 2)
    for unit in (1, 3, 4):
        rs_step(1, 1, unit)
    rs_step(1, 2, 0)
    rs_step(1, 1, 2)
    for unit in (1, 3, 4):
        rs_step(1, 2, unit)
    rs_step(1, 3, 0)
    rs_step(1, 2, 2)
    for unit in (1, 3, 4, 2):
        rs_step(1, 3, unit)

    def fin_copy(group):
        rows = pl.ds(*span(REDUCE[1], group))
        return rdma(fin_out.at[rows, :], fin_in.at[rows, :], sent.at[4], m_r.at[2 + group], partner)

    def sums_copy(group, k, crossing):
        ref = sums.at[c, z, :, pl.ds(*span(REDUCE[1], group))]
        return rdma(ref, ref, sent.at[4], s_r.at[group, crossing], at_z(k, other if crossing else c))

    routes = [(4, 0), (4, 1), (3, 0), (3, 1), (5, 0), (5, 1), (2, 0), (2, 1), (6, 0), (6, 1)]
    routes += [(1, 0), (1, 1), (7, 0), (7, 1), (0, 1)]
    for group in range(2):
        for unit in ((0, 1), (3, 4, 2))[group]:
            lo, size = REDUCE[1][unit]
            st[lo : lo + size, :] = rs_last(1, unit).astype(F32)
        lo, size = span(REDUCE[1], group)
        rows = pl.ds(lo, size)
        value = st[rows, :]
        square = jnp.sum(value * value, axis=1, keepdims=True)
        sums[c, z, :, lo : lo + size] = jnp.broadcast_to(square, (size, 128)).T[:8, :]
        for k, crossing in routes:
            start(sums_copy(group, k, crossing))
        fin_out[rows, :] = st[rows, other_cols].astype(BF16)
        start(fin_copy(group))

    def scale_of(core):
        total = jnp.sum(sums[core, :, 0, :], axis=0, keepdims=True)
        return lax.rsqrt(jnp.broadcast_to(total, (128, ROWS)).T[:, :1] / D + FLOOR)

    with jax.named_scope("sums"):
        for group in range(2):
            fin_copy(group).wait_recv()
            cols = pl.ds(*span(REDUCE[1], group))
            for crossing, ref in enumerate((sums.at[c, pl.ds(0, NZ - 1), :, cols], sums.at[other, :, :, cols])):
                rdma(ref, ref, sent.at[4], s_r.at[group, crossing], partner).wait_recv()
    out[own_rows, :] = st[:, own_cols] * scale_of(c) * gain_out[...]
    out[other_rows, :] = fin_in[...].astype(F32) * scale_of(other) * gain_out[...]
    with jax.named_scope("sends"):
        for kind, rows in enumerate(SENT_ROWS):
            ref = w_all.at[0, pl.ds(0, rows), pl.ds(0, WIDE)] if rows <= D else w_all.at[0, pl.ds(0, rows // 2), :]
            rdma(ref, ref, sent.at[kind], m_r.at[0], partner).wait_send()
        rdma(tap_all.at[c], tap_all.at[c], sent.at[5], m_r.at[1], partner).wait_send()


def per_device(residual_in, norm_gain, gate_proj, filter_proj, signal_proj, conv_taps, out_proj, final_gain):
    dma = pltpu.SemaphoreType.DMA
    return pl.pallas_call(
        kernel,
        out_shape=jax.ShapeDtypeStruct((2 * ROWS, COLS), F32),
        in_specs=[pl.BlockSpec(memory_space=pltpu.HBM)] * 8,
        out_specs=pl.BlockSpec(memory_space=pltpu.VMEM),
        scratch_shapes=[
            pltpu.VMEM((LAYERS, NZ, ROWS, PIECE), BF16),
            pltpu.VMEM((ROWS, COLS), BF16),
            pltpu.VMEM((NZ, ROWS, PIECE), BF16),
            pltpu.VMEM((LAYERS, D, 2 * WIDE), BF16),
            pltpu.VMEM((2 * CH, D), BF16),
            pltpu.VMEM((ROWS, 6 * CH), F32),
            pltpu.VMEM((8 + ROWS, 2 * CH), F32),
            pltpu.VMEM((ROWS, 2 * CH), BF16),
            pltpu.VMEM((ROWS, 128), F32),
            pltpu.VMEM((LAYERS, 2, 4, ROWS, PIECE), BF16),
            pltpu.VMEM((LAYERS, 2, 4, ROWS, PIECE), BF16),
            pltpu.VMEM((LAYERS, 2, 8, 2 * CH), F32),
            pltpu.VMEM((2, TAPS, LAYERS, CH), F32),
            pltpu.VMEM((LAYERS, D), F32),
            pltpu.VMEM((1, COLS), F32),
            pltpu.VMEM((2, NZ, 8, ROWS), F32),
            pltpu.VMEM((ROWS, PIECE), F32),
            pltpu.VMEM((ROWS, COLS), BF16),
            pltpu.VMEM((ROWS, COLS), BF16),
            dma((1,)),
            dma((6,)),
            dma((4 * UNITS,)),
            dma((3, 20)),
            dma((3, SIDE)),
            dma((4 * UNITS,)),
            dma((LAYERS,)),
            dma((2, 2)),
            dma((4,)),
        ],
        compiler_params=pltpu.CompilerParams(
            collective_id=0, has_side_effects=True, vmem_limit_bytes=44 * 1024 * 1024
        ),
    )(
        *(
            pltpu.with_memory_space_constraint(a, pltpu.HBM)
            for a in (
                residual_in, norm_gain, gate_proj, filter_proj, signal_proj, jnp.transpose(conv_taps, (1, 0, 2)),
                out_proj, final_gain.reshape(1, -1),
            )
        )
    )


def solution(mesh):
    return jax.shard_map(
        per_device,
        mesh=mesh,
        in_specs=(
            P("sp", "tp"),
            P(),
            P(None, "sp", "tp"),
            P(None, "sp", "tp"),
            P(None, "sp", "tp"),
            P(None, None, "tp"),
            P(None, "tp", "sp"),
            P("tp"),
        ),
        out_specs=P("sp", "tp"),
        check_vma=False,
    )
```

```python
import jax
import jax.numpy as jnp
from jax import lax
from jax.experimental import pallas as pl
from jax.experimental.pallas import tpu as pltpu
from jax.sharding import PartitionSpec as P

D = 4096
TAPS = 3
LAYERS = 2
FLOOR = 1e-06

NZ = 8
SIDE = 4
ROWS = 256
PIECE = 512
COLS = 256
CH = 128
WIDE = 512

F32 = jnp.float32
BF16 = jnp.bfloat16
MESH = pl.DeviceIdType.MESH

GATHER = (
    ((96, 80), (176, 80), (0, 16), (16, 48), (64, 32)),
    ((112, 80), (192, 64), (0, 16), (16, 48), (64, 48)),
)
REDUCE = (
    ((112, 80), (192, 64), (0, 16), (16, 48), (64, 48)),
    ((128, 64), (192, 64), (0, 16), (16, 64), (80, 48)),
)
GROUPS = ((0, 1), (2, 3, 4))
UNITS = 5
FAR = (0, 1, 1, 0, 1)

SENT_ROWS = (7680, 8192, 3584, 3584, 392)


def span(units, group):
    lo = units[GROUPS[group][0]][0]
    return lo, sum(units[u][1] for u in GROUPS[group])


def aligned(index, size):
    return pl.ds(pl.multiple_of(index * size, size), size)


def has(way, far, unit):
    return not far or FAR[unit] == way


def kernel(
    res, norm_gain, gate, filt, sig, taps, outp, final_gain, out,
    x_all, res_other, xg, w_all, w_out, acc, prod, mixed, sq, rs_out, rs_in, halo, tap_all, gain_in, gain_out,
    sums, st, fin_out, fin_in,
    loc, sent, ag_r, w_r, d_r, rs_r, h_r, s_r, m_r,
):
    s = lax.axis_index("sp")
    t = lax.axis_index("tp")
    z, c = t // 2, t % 2
    y, x = s // SIDE, s % SIDE
    other = 1 - c
    partner = (s, 2 * z + other)

    def at_z(k, core=None):
        return (s, ((z + k + NZ) % NZ) * 2 + (c if core is None else core))

    def at_x(k):
        return (y * SIDE + (x + k + SIDE) % SIDE, t)

    def at_y(k):
        return (((y + k + SIDE) % SIDE) * SIDE + x, t)

    half = 1 - c
    halo_next = ((s + half) % 16, 2 * z + other)

    def rdma(src, dst, send, recv, device):
        return pltpu.make_async_remote_copy(
            src_ref=src, dst_ref=dst, send_sem=send, recv_sem=recv, device_id=device, device_id_type=MESH
        )

    def start(copy):
        copy.start()

    barrier = pltpu.get_barrier_semaphore()
    peers = [at_z(1), at_z(-1), at_z(1, other), at_z(-1, other), at_x(1), at_x(-1), at_y(1), at_y(-1), partner]
    for peer in peers:
        pl.semaphore_signal(barrier, inc=1, device_id=peer, device_id_type=MESH)

    own_cols = aligned(c, COLS)
    other_cols = aligned(other, COLS)
    own_rows = aligned(half, ROWS)
    other_rows = aligned(1 - half, ROWS)

    local = []

    def place(src, dst):
        copy = pltpu.make_async_copy(src, dst, loc.at[0])
        copy.start()
        local.append(copy)

    place(res.at[own_rows, :], x_all.at[0, z, :, own_cols])
    place(res.at[other_rows, :], res_other)
    for l in range(LAYERS):
        for part, ref in enumerate((gate, filt, sig)):
            first = pl.multiple_of(c * 3 * CH + (part + 1) * CH, CH)
            place(ref.at[l], w_all.at[l, aligned(s, 256), pl.ds(first, CH)])
        for h in range(2):
            place(
                outp.at[l, :, pl.ds(h * CH, CH)],
                w_all.at[l, aligned(2 * s + h, CH), aligned(c * 7, CH)],
            )
    place(norm_gain, gain_in)
    place(taps, tap_all.at[c])
    place(final_gain, gain_out)

    with jax.named_scope("barrier"):
        pl.semaphore_wait(barrier, len(peers))
    with jax.named_scope("local"):
        for copy in local:
            copy.wait()

    def lanes(what, core):
        if what == "proj":
            return pl.ds(pl.multiple_of(core * 3 * CH + CH, CH), 3 * CH)
        if what == "out":
            return aligned(core * 7, CH)
        return aligned(core, WIDE)

    carriers = ((0, "proj", 0, 64), (0, "proj", 64, 64), (0, "out", 0, 128), (1, "both", 0, 128))

    def w_copy(carrier, group, half, axis, across, sign, fwd, sending):
        l, what, first, size = carriers[carrier]
        step = sign if fwd else 0
        along = -step if sending else -step - sign
        lo = half * 128 + first
        if fwd:
            size = size // 2
            lo += 0 if sign == 1 else size
        if axis == 0:
            yy, xx = y + across, x + along
        else:
            yy, xx = y + along, x + across
        index = ((yy + SIDE) % SIDE) * SIDE + (xx + SIDE) % SIDE
        ref = w_all.at[l, pl.ds(pl.multiple_of(index * 256 + lo, 32), size), lanes(what, c)]
        slot = group * 2 + (1 if fwd else 0)
        device = at_x(sign) if axis == 0 else at_y(sign)
        return rdma(ref, ref, sent.at[0], w_r.at[carrier % 3, slot], device)

    groups = {("a", 1): (0, 0, 0, 0), ("b", 1): (5, 1, 1, 0)}
    for i, p in enumerate((0, -1, 1, 2)):
        groups["a", 2, p] = (1 + i, 0, 1, p)
        groups["b", 2, p] = (6 + i, 1, 0, p)

    def w_send(carrier, *name):
        group, half, axis, across = groups[name]
        for sign in (1, -1):
            start(w_copy(carrier, group, half, axis, across, sign, False, True))

    def w_wait(carrier, group, fwd):
        l, what, _, size = carriers[carrier]
        ref = w_all.at[l, pl.ds(0, size if fwd else 2 * size), lanes(what, c)]
        rdma(ref, ref, sent.at[0], w_r.at[carrier % 3, group * 2 + (1 if fwd else 0)], partner).wait_recv()

    def w_forward(carrier, *name):
        group, half, axis, across = groups[name]
        w_wait(carrier, group, False)
        for sign in (1, -1):
            start(w_copy(carrier, group, half, axis, across, sign, True, True))

    def w_finish(carrier, *name):
        w_wait(carrier, groups[name][0], True)

    parcels = ((0, "proj"), (0, "out"), (1, "both"))

    def w_parcel(parcel, k, core):
        l, what = parcels[parcel]
        ref = w_all.at[l, aligned((y + k + SIDE) % SIDE, 1024), lanes(what, core)]
        slot = (k + SIDE) % SIDE
        return rdma(ref, ref, sent.at[1], d_r.at[parcel, slot], partner)

    def w_hand(parcel, *ks):
        for k in ks:
            start(w_parcel(parcel, k, c))

    def w_taken(parcel, k):
        with jax.named_scope(f"taken#p={parcel}#k={k}"):
            w_parcel(parcel, k, other).wait_recv()

    def w_stage(carrier, stage):
        with jax.named_scope(f"w#t={carrier}#s={stage}"):
            w_stage_body(carrier, stage)

    def w_stage_body(t, stage):
        if stage == 0:
            w_send(t, "a", 1)
            w_send(t, "b", 1)
            w_send(t, "b", 2, 0)
            w_send(t, "a", 2, 0)
        elif stage == 1:
            w_forward(t, "a", 1)
            w_forward(t, "b", 1)
            for p in (-1, 1):
                w_send(t, "a", 2, p)
                w_send(t, "b", 2, p)
            w_forward(t, "b", 2, 0)
            w_forward(t, "a", 2, 0)
        elif stage == 2:
            w_finish(t, "a", 1)
            w_send(t, "a", 2, 2)
            w_finish(t, "b", 1)
            w_send(t, "b", 2, 2)
        elif stage == 3:
            for p in (-1, 1):
                w_forward(t, "a", 2, p)
                w_forward(t, "b", 2, p)
        else:
            w_forward(t, "a", 2, 2)
            w_forward(t, "b", 2, 2)

    def w_end(parcel, *ks):
        with jax.named_scope(f"end#p={parcel}#k={ks[0]}"):
            for k in ks:
                for t in ((0, 1), (2,), (3,))[parcel]:
                    w_finish(t, "a", 2, k)
                    w_finish(t, "b", 2, k)
        w_hand(parcel, *ks)

    def build_w_out(l, k):
        first = ((y + k + SIDE) % SIDE) * 8

        def body(i, carry):
            for core in range(2):
                w_out[core * CH : (core + 1) * CH, aligned(first + i, CH)] = w_all[
                    l, aligned(first + i, CH), core * 7 * CH : (core * 7 + 1) * CH
                ]
            return carry

        lax.fori_loop(0, 8, body, 0)

    def chunk_at(k):
        return (z + k + NZ) % NZ

    def ag_copy(l, way, dist, unit):
        sign = 1 - 2 * way
        lo, size = GATHER[l][unit]
        ref = x_all.at[l, chunk_at(-sign * dist), pl.ds(lo, size), :]
        return rdma(ref, ref, sent.at[2], ag_r.at[dist * UNITS + unit], at_z(sign))

    def first_copy(way, unit, crossing):
        lo, size = GATHER[0][unit]
        dst = x_all.at[0, z, pl.ds(lo, size), own_cols]
        src = res_other.at[pl.ds(lo, size), :] if crossing else dst
        return rdma(src, dst, sent.at[2], ag_r.at[unit], at_z(1 - 2 * way, other if crossing else c))

    def ag_first(l, unit):
        for way in range(2):
            if l == 0:
                start(first_copy(way, unit, False))
                start(first_copy(way, unit, True))
            else:
                start(ag_copy(l, way, 0, unit))

    def ag_step(l, dist, unit):
        with jax.named_scope(f"ag#l={l}#d={dist}#u={unit}"):
            _, size = GATHER[l][unit]
            ref = x_all.at[l, 0, pl.ds(0, size if dist == 3 else 2 * size), :]
            rdma(ref, ref, sent.at[2], ag_r.at[dist * UNITS + unit], partner).wait_recv()
            for way in range(2):
                if dist < 3 and has(way, dist == 2, unit):
                    start(ag_copy(l, way, dist + 1, unit))

    def take(l, group, chunk):
        take_rows(l, span(GATHER[l], group), chunk)

    def take_rows(l, which, chunk):
        lo, size = which
        rows = pl.ds(lo, size)
        value = x_all[l, chunk, rows, :].astype(F32)
        square = value * value
        total = square[:, :128]
        for i in range(1, PIECE // 128):
            total = total + square[:, i * 128 : (i + 1) * 128]
        sq[rows, :] += total
        xg[chunk, rows, :] = (value * gain_in[l : l + 1, aligned(chunk, PIECE)]).astype(BF16)

    def arrived_at(dist):
        return (-dist - 1, dist + 1) if dist < 3 else (4,)

    def multiply(l, group, chunk):
        multiply_rows(l, span(GATHER[l], group), chunk)

    def multiply_rows(l, which, chunk):
        lo, size = which
        acc[lo : lo + size, :] += jnp.dot(
            xg[chunk, lo : lo + size, :],
            w_all[l, aligned(chunk, PIECE), CH : 7 * CH],
            preferred_element_type=F32,
        )

    def multiply_row(l, group, k):
        first = ((y + k + SIDE) % SIDE) * 2
        with jax.named_scope(f"mult#g={group}"):
            multiply(l, group, first)
            multiply(l, group, first + 1)

    def start_sums():
        sq[...] = jnp.zeros_like(sq)
        acc[...] = jnp.zeros_like(acc)

    def gates(l, group):
        gates_rows(l, span(GATHER[l], group))

    def gates_rows(l, which):
        lo, size = which
        rows = pl.ds(lo, size)
        mean = jnp.sum(sq[rows, :], axis=1, keepdims=True) / D
        scale = lax.rsqrt(mean + FLOOR)
        for core in range(2):
            base = core * 3 * CH
            value = (acc[rows, base + CH : base + 2 * CH] * scale) * (acc[rows, base + 2 * CH : base + 3 * CH] * scale)
            prod[pl.ds(8 + lo, size), core * CH : (core + 1) * CH] = value.astype(BF16).astype(F32)
            acc[rows, base : base + CH] = acc[rows, base : base + CH] * scale

    def mix(l, unit):
        lo, size = REDUCE[l][unit]
        rows = pl.ds(lo, size)
        for core in range(2):
            cols = pl.ds(core * CH, CH)
            filtered = jnp.zeros((size, CH), F32)
            for k in range(TAPS):
                tap = tap_all[core, k, l : l + 1, :]
                filtered = filtered + tap * prod[pl.ds(8 + lo - (TAPS - 1) + k, size), cols]
            gated = acc[rows, core * 3 * CH : core * 3 * CH + CH]
            mixed[rows, cols] = (gated * filtered).astype(BF16)

    def halo_copy(l):
        return rdma(halo.at[l, 0], halo.at[l, 1], sent.at[4], h_r.at[l], halo_next)

    def give_halo(l):
        halo[l, 0] = prod[ROWS:, :]
        start(halo_copy(l))

    def take_halo(l):
        with jax.named_scope("halo"):
            halo_copy(l).wait_recv()
        first = jnp.logical_and(s == 0, half == 0)
        prod[:8, :] = jnp.where(first, 0.0, halo[l, 1])

    def rs_copy(l, i, way, k, unit):
        lo, size = REDUCE[l][unit]
        rows = pl.ds(lo, size)
        return rdma(
            rs_out.at[l, way, k - 1, rows, :], rs_in.at[l, way, k - 1, rows, :],
            sent.at[3], rs_r.at[i * UNITS + unit], at_z(1 - 2 * way),
        )

    def partial(l, unit, chunk):
        lo, size = REDUCE[l][unit]
        return jnp.dot(mixed[lo : lo + size, :], w_out[:, aligned(chunk, PIECE)], preferred_element_type=F32)

    def rs_wait(l, i, unit):
        _, size = REDUCE[l][unit]
        ref = rs_in.at[l, 0, 0, pl.ds(0, size if i == 3 else 2 * size), :]
        rdma(ref, ref, sent.at[3], rs_r.at[i * UNITS + unit], partner).wait_recv()

    def arrived(l, way, k, unit):
        lo, size = REDUCE[l][unit]
        return rs_in[l, way, k - 1, lo : lo + size, :].astype(F32)

    def rs_step(l, i, unit):
        with jax.named_scope(f"rs#l={l}#i={i}#u={unit}"):
            lo, size = REDUCE[l][unit]
            if i > 0:
                rs_wait(l, i - 1, unit)
            for way in range(2):
                k = 4 - i if has(way, True, unit) else 3 - i
                if k < 1:
                    continue
                value = partial(l, unit, chunk_at(k * (1 - 2 * way)))
                if i > 0:
                    value = value + arrived(l, way, k + 1, unit)
                rs_out[l, way, k - 1, lo : lo + size, :] = value.astype(BF16)
                start(rs_copy(l, i, way, k, unit))

    def rs_last(l, unit):
        with jax.named_scope(f"last#l={l}#u={unit}"):
            lo, size = REDUCE[l][unit]
            value = partial(l, unit, z)
            rs_wait(l, 3, unit)
            for way in range(2):
                value = value + arrived(l, way, 1, unit)
            return (x_all[l, z, lo : lo + size, :].astype(F32) + value).astype(BF16)

    def take_step(l, group, dist):
        for k in arrived_at(dist):
            take(l, group, chunk_at(k))
            if l == 1:
                multiply(l, group, chunk_at(k))

    ag_first(0, 0)
    ag_first(0, 1)
    w_stage(0, 0)
    w_stage(1, 0)
    start(rdma(res_other, x_all.at[0, z, :, own_cols], sent.at[4], m_r.at[0], partner))
    start(rdma(tap_all.at[c], tap_all.at[c], sent.at[5], m_r.at[1], partner))
    for unit in (3, 4, 2):
        ag_first(0, unit)
    start_sums()
    rdma(res_other, x_all.at[0, z, :, other_cols], sent.at[4], m_r.at[0], partner).wait_recv()
    take(0, 0, z)
    take(0, 1, z)

    w_stage(2, 0)
    w_stage(0, 1)
    ag_step(0, 0, 0)
    w_stage(1, 1)
    ag_step(0, 0, 1)
    take_step(0, 0, 0)
    ag_step(0, 0, 3)
    ag_step(0, 0, 4)
    w_stage(0, 2)
    ag_step(0, 0, 2)
    take_step(0, 1, 0)
    w_stage(2, 1)
    ag_step(0, 1, 0)
    w_stage(1, 2)
    w_stage(0, 3)
    ag_step(0, 1, 1)
    take_step(0, 0, 1)
    ag_step(0, 1, 3)
    ag_step(0, 1, 4)
    w_stage(1, 3)
    ag_step(0, 1, 2)
    take_step(0, 1, 1)
    w_stage(0, 4)
    ag_step(0, 2, 0)
    ag_step(0, 2, 1)
    take_step(0, 0, 2)
    w_stage(2, 2)
    w_stage(1, 4)
    ag_step(0, 2, 3)
    ag_step(0, 2, 4)
    w_end(0, 0)
    w_stage(2, 3)
    ag_step(0, 2, 2)
    take_step(0, 1, 2)
    w_end(0, -1, 1)
    ag_step(0, 3, 0)
    w_stage(2, 4)
    w_end(1, 0)
    ag_step(0, 3, 1)
    take_step(0, 0, 3)
    w_end(0, 2)
    w_taken(0, 0)
    multiply_row(0, 0, 0)
    for unit in (3, 4, 2):
        ag_step(0, 3, unit)
    take_step(0, 1, 3)
    w_end(1, -1, 1)
    w_taken(0, -1)
    multiply_row(0, 0, -1)
    w_taken(1, 0)
    build_w_out(0, 0)
    w_end(1, 2)
    w_stage(3, 0)
    w_taken(0, 1)
    multiply_row(0, 0, 1)
    for k in (-1, 1):
        w_taken(1, k)
        build_w_out(0, k)
    w_taken(0, 2)
    multiply_row(0, 0, 2)
    gates(0, 0)
    rdma(tap_all.at[other], tap_all.at[other], sent.at[4], m_r.at[1], partner).wait_recv()
    give_halo(0)
    mix(0, 0)
    mix(0, 1)
    w_taken(1, 2)
    build_w_out(0, 2)

    rs_step(0, 0, 0)
    rs_step(0, 0, 1)
    for k in (0, -1, 1, 2):
        multiply_row(0, 1, k)
    gates(0, 1)
    for unit in (3, 4):
        mix(0, unit)
        rs_step(0, 0, unit)
    rs_step(0, 1, 0)
    take_halo(0)
    mix(0, 2)
    rs_step(0, 0, 2)
    start_sums()
    for unit in (1, 3, 4):
        rs_step(0, 1, unit)
    w_stage(3, 1)
    rs_step(0, 2, 0)
    rs_step(0, 1, 2)
    for unit in (1, 3, 4):
        rs_step(0, 2, unit)
    rs_step(0, 3, 0)
    rs_step(0, 2, 2)
    w_stage(3, 2)
    for unit in (1, 3, 4):
        rs_step(0, 3, unit)

    def next_stream(unit):
        lo, size = REDUCE[0][unit]
        x_all[1, z, lo : lo + size, :] = rs_last(0, unit)
        ag_first(1, unit)

    next_stream(0)
    rs_step(0, 3, 2)
    w_stage(3, 3)
    next_stream(1)
    take(1, 0, z)
    next_stream(3)
    next_stream(4)

    ag_step(1, 0, 0)
    w_stage(3, 4)
    next_stream(2)
    take(1, 1, z)
    ag_step(1, 0, 1)
    ag_step(1, 0, 3)
    w_end(2, 0)
    w_end(2, -1, 1)
    ag_step(1, 0, 4)
    ag_step(1, 0, 2)
    ag_step(1, 1, 0)
    ag_step(1, 1, 1)
    w_end(2, 2)
    for unit in (3, 4, 2):
        ag_step(1, 1, unit)
    for k in (0, -1, 1, 2):
        w_taken(2, k)
        build_w_out(1, k)
    ag_step(1, 2, 0)
    for group in range(2):
        multiply(1, group, z)
        take_step(1, group, 0)
    ag_step(1, 2, 1)
    take_step(1, 0, 1)
    ag_step(1, 2, 3)
    take_step(1, 1, 1)
    ag_step(1, 2, 4)
    ag_step(1, 2, 2)
    take_step(1, 0, 2)
    take_step(1, 1, 2)
    for unit in (0, 1):
        ag_step(1, 3, unit)
        take_rows(1, GATHER[1][unit], chunk_at(4))
        multiply_rows(1, GATHER[1][unit], chunk_at(4))
        gates_rows(1, GATHER[1][unit])
        if unit == 1:
            give_halo(1)
        mix(1, unit)
        rs_step(1, 0, unit)
    for unit in (3, 4, 2):
        ag_step(1, 3, unit)
    take_step(1, 1, 3)
    gates(1, 1)
    for unit in (3, 4):
        mix(1, unit)
        rs_step(1, 0, unit)
    rs_step(1, 1, 0)
    take_halo(1)
    mix(1, 2)
    rs_step(1, 0, 2)
    for unit in (1, 3, 4):
        rs_step(1, 1, unit)
    rs_step(1, 2, 0)
    rs_step(1, 1, 2)
    for unit in (1, 3, 4):
        rs_step(1, 2, unit)
    rs_step(1, 3, 0)
    rs_step(1, 2, 2)
    for unit in (1, 3, 4, 2):
        rs_step(1, 3, unit)

    def fin_copy(group):
        rows = pl.ds(*span(REDUCE[1], group))
        return rdma(fin_out.at[rows, :], fin_in.at[rows, :], sent.at[4], m_r.at[2 + group], partner)

    def sums_copy(group, k, crossing):
        ref = sums.at[c, z, :, pl.ds(*span(REDUCE[1], group))]
        return rdma(ref, ref, sent.at[4], s_r.at[group, crossing], at_z(k, other if crossing else c))

    routes = [(4, 0), (4, 1), (3, 0), (3, 1), (5, 0), (5, 1), (2, 0), (2, 1), (6, 0), (6, 1)]
    routes += [(1, 0), (1, 1), (7, 0), (7, 1), (0, 1)]
    for group in range(2):
        for unit in ((0, 1), (3, 4, 2))[group]:
            lo, size = REDUCE[1][unit]
            st[lo : lo + size, :] = rs_last(1, unit).astype(F32)
        lo, size = span(REDUCE[1], group)
        rows = pl.ds(lo, size)
        value = st[rows, :]
        square = jnp.sum(value * value, axis=1, keepdims=True)
        sums[c, z, :, lo : lo + size] = jnp.broadcast_to(square, (size, 128)).T[:8, :]
        for k, crossing in routes:
            start(sums_copy(group, k, crossing))
        fin_out[rows, :] = st[rows, other_cols].astype(BF16)
        start(fin_copy(group))

    def scale_of(core):
        total = jnp.sum(sums[core, :, 0, :], axis=0, keepdims=True)
        return lax.rsqrt(jnp.broadcast_to(total, (128, ROWS)).T[:, :1] / D + FLOOR)

    with jax.named_scope("sums"):
        for group in range(2):
            fin_copy(group).wait_recv()
            cols = pl.ds(*span(REDUCE[1], group))
            for crossing, ref in enumerate((sums.at[c, pl.ds(0, NZ - 1), :, cols], sums.at[other, :, :, cols])):
                rdma(ref, ref, sent.at[4], s_r.at[group, crossing], partner).wait_recv()
    out[own_rows, :] = st[:, own_cols] * scale_of(c) * gain_out[...]
    out[other_rows, :] = fin_in[...].astype(F32) * scale_of(other) * gain_out[...]
    with jax.named_scope("sends"):
        for kind, rows in enumerate(SENT_ROWS):
            ref = w_all.at[0, pl.ds(0, rows), pl.ds(0, WIDE)] if rows <= D else w_all.at[0, pl.ds(0, rows // 2), :]
            rdma(ref, ref, sent.at[kind], m_r.at[0], partner).wait_send()
        rdma(tap_all.at[c], tap_all.at[c], sent.at[5], m_r.at[1], partner).wait_send()


def per_device(residual_in, norm_gain, gate_proj, filter_proj, signal_proj, conv_taps, out_proj, final_gain):
    dma = pltpu.SemaphoreType.DMA
    return pl.pallas_call(
        kernel,
        out_shape=jax.ShapeDtypeStruct((2 * ROWS, COLS), F32),
        in_specs=[pl.BlockSpec(memory_space=pltpu.HBM)] * 8,
        out_specs=pl.BlockSpec(memory_space=pltpu.VMEM),
        scratch_shapes=[
            pltpu.VMEM((LAYERS, NZ, ROWS, PIECE), BF16),
            pltpu.VMEM((ROWS, COLS), BF16),
            pltpu.VMEM((NZ, ROWS, PIECE), BF16),
            pltpu.VMEM((LAYERS, D, 2 * WIDE), BF16),
            pltpu.VMEM((2 * CH, D), BF16),
            pltpu.VMEM((ROWS, 6 * CH), F32),
            pltpu.VMEM((8 + ROWS, 2 * CH), F32),
            pltpu.VMEM((ROWS, 2 * CH), BF16),
            pltpu.VMEM((ROWS, 128), F32),
            pltpu.VMEM((LAYERS, 2, 4, ROWS, PIECE), BF16),
            pltpu.VMEM((LAYERS, 2, 4, ROWS, PIECE), BF16),
            pltpu.VMEM((LAYERS, 2, 8, 2 * CH), F32),
            pltpu.VMEM((2, TAPS, LAYERS, CH), F32),
            pltpu.VMEM((LAYERS, D), F32),
            pltpu.VMEM((1, COLS), F32),
            pltpu.VMEM((2, NZ, 8, ROWS), F32),
            pltpu.VMEM((ROWS, PIECE), F32),
            pltpu.VMEM((ROWS, COLS), BF16),
            pltpu.VMEM((ROWS, COLS), BF16),
            dma((1,)),
            dma((6,)),
            dma((4 * UNITS,)),
            dma((3, 20)),
            dma((3, SIDE)),
            dma((4 * UNITS,)),
            dma((LAYERS,)),
            dma((2, 2)),
            dma((4,)),
        ],
        compiler_params=pltpu.CompilerParams(
            collective_id=0, has_side_effects=True, vmem_limit_bytes=44 * 1024 * 1024
        ),
    )(
        *(
            pltpu.with_memory_space_constraint(a, pltpu.HBM)
            for a in (
                residual_in, norm_gain, gate_proj, filter_proj, signal_proj, jnp.transpose(conv_taps, (1, 0, 2)),
                out_proj, final_gain.reshape(1, -1),
            )
        )
    )


def solution(mesh):
    return jax.shard_map(
        per_device,
        mesh=mesh,
        in_specs=(
            P("sp", "tp"),
            P(),
            P(None, "sp", "tp"),
            P(None, "sp", "tp"),
            P(None, "sp", "tp"),
            P(None, None, "tp"),
            P(None, "tp", "sp"),
            P("tp"),
        ),
        out_specs=P("sp", "tp"),
        check_vma=False,
    )
```

```python
import jax
import jax.numpy as jnp
from jax import lax
from jax.experimental import pallas as pl
from jax.experimental.pallas import tpu as pltpu
from jax.sharding import PartitionSpec as P

D = 4096
TAPS = 3
LAYERS = 2
FLOOR = 1e-06

NZ = 8
SIDE = 4
ROWS = 256
PIECE = 512
COLS = 256
CH = 128
WIDE = 512

F32 = jnp.float32
BF16 = jnp.bfloat16
MESH = pl.DeviceIdType.MESH

GATHER = (
    ((96, 80), (176, 80), (0, 16), (16, 48), (64, 32)),
    ((112, 80), (192, 64), (0, 16), (16, 48), (64, 48)),
)
REDUCE = (
    ((112, 80), (192, 64), (0, 16), (16, 48), (64, 48)),
    ((128, 64), (192, 64), (0, 16), (16, 64), (80, 48)),
)
GROUPS = ((0, 1), (2, 3, 4))
UNITS = 5
FAR = (0, 1, 1, 0, 1)

SENT_ROWS = (7680, 8192, 3584, 3584, 392)


def span(units, group):
    lo = units[GROUPS[group][0]][0]
    return lo, sum(units[u][1] for u in GROUPS[group])


def aligned(index, size):
    return pl.ds(pl.multiple_of(index * size, size), size)


def has(way, far, unit):
    return not far or FAR[unit] == way


def kernel(
    res, norm_gain, gate, filt, sig, taps, outp, final_gain, out,
    x_all, res_other, xg, w_all, w_out, acc, prod, mixed, sq, rs_out, rs_in, halo, tap_all, gain_in, gain_out,
    sums, st, fin_out, fin_in,
    loc, sent, ring_r, w_r, d_r, h_r, s_r, m_r,
):
    s = lax.axis_index("sp")
    t = lax.axis_index("tp")
    z, c = t // 2, t % 2
    y, x = s // SIDE, s % SIDE
    other = 1 - c
    partner = (s, 2 * z + other)

    def at_z(k, core=None):
        return (s, ((z + k + NZ) % NZ) * 2 + (c if core is None else core))

    def at_x(k):
        return (y * SIDE + (x + k + SIDE) % SIDE, t)

    def at_y(k):
        return (((y + k + SIDE) % SIDE) * SIDE + x, t)

    half = 1 - c
    halo_next = ((s + half) % 16, 2 * z + other)

    def rdma(src, dst, send, recv, device):
        return pltpu.make_async_remote_copy(
            src_ref=src, dst_ref=dst, send_sem=send, recv_sem=recv, device_id=device, device_id_type=MESH
        )

    def start(copy):
        copy.start()

    barrier = pltpu.get_barrier_semaphore()
    peers = [at_z(1), at_z(-1), at_z(1, other), at_z(-1, other), at_x(1), at_x(-1), at_y(1), at_y(-1), partner]
    for peer in peers:
        pl.semaphore_signal(barrier, inc=1, device_id=peer, device_id_type=MESH)

    own_cols = aligned(c, COLS)
    other_cols = aligned(other, COLS)
    own_rows = aligned(half, ROWS)
    other_rows = aligned(1 - half, ROWS)

    local = []

    def place(src, dst):
        copy = pltpu.make_async_copy(src, dst, loc.at[0])
        copy.start()
        local.append(copy)

    place(res.at[own_rows, :], x_all.at[0, z, :, own_cols])
    place(res.at[other_rows, :], res_other)
    for l in range(LAYERS):
        for part, ref in enumerate((gate, filt, sig)):
            first = pl.multiple_of(c * 3 * CH + (part + 1) * CH, CH)
            place(ref.at[l], w_all.at[l, aligned(s, 256), pl.ds(first, CH)])
        for h in range(2):
            place(
                outp.at[l, :, pl.ds(h * CH, CH)],
                w_all.at[l, aligned(2 * s + h, CH), aligned(c * 7, CH)],
            )
    place(norm_gain, gain_in)
    place(taps, tap_all.at[c])
    place(final_gain, gain_out)

    with jax.named_scope("barrier"):
        pl.semaphore_wait(barrier, len(peers))
    with jax.named_scope("local"):
        for copy in local:
            copy.wait()

    def lanes(what, core):
        if what == "proj":
            return pl.ds(pl.multiple_of(core * 3 * CH + CH, CH), 3 * CH)
        if what == "out":
            return aligned(core * 7, CH)
        return aligned(core, WIDE)

    carriers = ((0, "proj", 0, 64), (0, "proj", 64, 64), (0, "out", 0, 128), (1, "both", 0, 128))

    def w_copy(carrier, group, half, axis, across, sign, fwd, sending):
        l, what, first, size = carriers[carrier]
        step = sign if fwd else 0
        along = -step if sending else -step - sign
        lo = half * 128 + first
        if fwd:
            size = size // 2
            lo += 0 if sign == 1 else size
        if axis == 0:
            yy, xx = y + across, x + along
        else:
            yy, xx = y + along, x + across
        index = ((yy + SIDE) % SIDE) * SIDE + (xx + SIDE) % SIDE
        ref = w_all.at[l, pl.ds(pl.multiple_of(index * 256 + lo, 32), size), lanes(what, c)]
        slot = group * 2 + (1 if fwd else 0)
        device = at_x(sign) if axis == 0 else at_y(sign)
        return rdma(ref, ref, sent.at[0], w_r.at[carrier % 3, slot], device)

    groups = {("a", 1): (0, 0, 0, 0), ("b", 1): (5, 1, 1, 0)}
    for i, p in enumerate((0, -1, 1, 2)):
        groups["a", 2, p] = (1 + i, 0, 1, p)
        groups["b", 2, p] = (6 + i, 1, 0, p)

    def w_send(carrier, *name):
        group, half, axis, across = groups[name]
        for sign in (1, -1):
            start(w_copy(carrier, group, half, axis, across, sign, False, True))

    def w_wait(carrier, group, fwd):
        l, what, _, size = carriers[carrier]
        ref = w_all.at[l, pl.ds(0, size if fwd else 2 * size), lanes(what, c)]
        rdma(ref, ref, sent.at[0], w_r.at[carrier % 3, group * 2 + (1 if fwd else 0)], partner).wait_recv()

    def w_forward(carrier, *name):
        group, half, axis, across = groups[name]
        w_wait(carrier, group, False)
        for sign in (1, -1):
            start(w_copy(carrier, group, half, axis, across, sign, True, True))

    def w_finish(carrier, *name):
        w_wait(carrier, groups[name][0], True)

    parcels = ((0, "proj"), (0, "out"), (1, "both"))

    def w_parcel(parcel, k, core):
        l, what = parcels[parcel]
        ref = w_all.at[l, aligned((y + k + SIDE) % SIDE, 1024), lanes(what, core)]
        slot = (k + SIDE) % SIDE
        return rdma(ref, ref, sent.at[1], d_r.at[parcel, slot], partner)

    def w_hand(parcel, *ks):
        for k in ks:
            start(w_parcel(parcel, k, c))

    def w_taken(parcel, k):
        with jax.named_scope(f"taken#p={parcel}#k={k}"):
            w_parcel(parcel, k, other).wait_recv()

    def w_stage(carrier, stage):
        with jax.named_scope(f"w#t={carrier}#s={stage}"):
            w_stage_body(carrier, stage)

    def w_stage_body(t, stage):
        if stage == 0:
            w_send(t, "a", 1)
            w_send(t, "b", 1)
            w_send(t, "b", 2, 0)
            w_send(t, "a", 2, 0)
        elif stage == 1:
            w_forward(t, "a", 1)
            w_forward(t, "b", 1)
            for p in (-1, 1):
                w_send(t, "a", 2, p)
                w_send(t, "b", 2, p)
            w_forward(t, "b", 2, 0)
            w_forward(t, "a", 2, 0)
        elif stage == 2:
            w_finish(t, "a", 1)
            w_send(t, "a", 2, 2)
            w_finish(t, "b", 1)
            w_send(t, "b", 2, 2)
        elif stage == 3:
            for p in (-1, 1):
                w_forward(t, "a", 2, p)
                w_forward(t, "b", 2, p)
        else:
            w_forward(t, "a", 2, 2)
            w_forward(t, "b", 2, 2)

    def w_end(parcel, *ks):
        with jax.named_scope(f"end#p={parcel}#k={ks[0]}"):
            for k in ks:
                for t in ((0, 1), (2,), (3,))[parcel]:
                    w_finish(t, "a", 2, k)
                    w_finish(t, "b", 2, k)
        w_hand(parcel, *ks)

    def build_w_out(l, k):
        first = ((y + k + SIDE) % SIDE) * 8

        def body(i, carry):
            for core in range(2):
                w_out[core * CH : (core + 1) * CH, aligned(first + i, CH)] = w_all[
                    l, aligned(first + i, CH), core * 7 * CH : (core * 7 + 1) * CH
                ]
            return carry

        lax.fori_loop(0, 8, body, 0)

    def chunk_at(k):
        return (z + k + NZ) % NZ

    def ag_copy(l, way, dist, unit):
        sign = 1 - 2 * way
        lo, size = GATHER[l][unit]
        ref = x_all.at[l, chunk_at(-sign * dist), pl.ds(lo, size), :]
        return rdma(ref, ref, sent.at[2], ring_r.at[dist * UNITS + unit], at_z(sign))

    def first_copy(way, unit, crossing):
        lo, size = GATHER[0][unit]
        dst = x_all.at[0, z, pl.ds(lo, size), own_cols]
        src = res_other.at[pl.ds(lo, size), :] if crossing else dst
        return rdma(src, dst, sent.at[2], ring_r.at[unit], at_z(1 - 2 * way, other if crossing else c))

    def ag_first(l, unit):
        for way in range(2):
            if l == 0:
                start(first_copy(way, unit, False))
                start(first_copy(way, unit, True))
            else:
                start(ag_copy(l, way, 0, unit))

    def ag_step(l, dist, unit):
        with jax.named_scope(f"ag#l={l}#d={dist}#u={unit}"):
            _, size = GATHER[l][unit]
            ref = x_all.at[l, 0, pl.ds(0, size if dist == 3 else 2 * size), :]
            rdma(ref, ref, sent.at[2], ring_r.at[dist * UNITS + unit], partner).wait_recv()
            for way in range(2):
                if dist < 3 and has(way, dist == 2, unit):
                    start(ag_copy(l, way, dist + 1, unit))

    def take(l, group, chunk):
        take_rows(l, span(GATHER[l], group), chunk)

    def take_rows(l, which, chunk):
        lo, size = which
        rows = pl.ds(lo, size)
        value = x_all[l, chunk, rows, :].astype(F32)
        square = value * value
        total = square[:, :128]
        for i in range(1, PIECE // 128):
            total = total + square[:, i * 128 : (i + 1) * 128]
        sq[rows, :] += total
        xg[chunk, rows, :] = (value * gain_in[l : l + 1, aligned(chunk, PIECE)]).astype(BF16)

    def arrived_at(dist):
        return (-dist - 1, dist + 1) if dist < 3 else (4,)

    def multiply(l, group, chunk):
        multiply_rows(l, span(GATHER[l], group), chunk)

    def multiply_rows(l, which, chunk):
        lo, size = which
        acc[lo : lo + size, :] += jnp.dot(
            xg[chunk, lo : lo + size, :],
            w_all[l, aligned(chunk, PIECE), CH : 7 * CH],
            preferred_element_type=F32,
        )

    def multiply_row(l, group, k):
        first = ((y + k + SIDE) % SIDE) * 2
        with jax.named_scope(f"mult#g={group}"):
            multiply(l, group, first)
            multiply(l, group, first + 1)

    def start_sums():
        sq[...] = jnp.zeros_like(sq)
        acc[...] = jnp.zeros_like(acc)

    def gates(l, group):
        gates_rows(l, span(GATHER[l], group))

    def gates_rows(l, which):
        lo, size = which
        rows = pl.ds(lo, size)
        mean = jnp.sum(sq[rows, :], axis=1, keepdims=True) / D
        scale = lax.rsqrt(mean + FLOOR)
        for core in range(2):
            base = core * 3 * CH
            value = (acc[rows, base + CH : base + 2 * CH] * scale) * (acc[rows, base + 2 * CH : base + 3 * CH] * scale)
            prod[pl.ds(8 + lo, size), core * CH : (core + 1) * CH] = value.astype(BF16).astype(F32)
            acc[rows, base : base + CH] = acc[rows, base : base + CH] * scale

    def mix(l, unit):
        lo, size = REDUCE[l][unit]
        rows = pl.ds(lo, size)
        for core in range(2):
            cols = pl.ds(core * CH, CH)
            filtered = jnp.zeros((size, CH), F32)
            for k in range(TAPS):
                tap = tap_all[core, k, l : l + 1, :]
                filtered = filtered + tap * prod[pl.ds(8 + lo - (TAPS - 1) + k, size), cols]
            gated = acc[rows, core * 3 * CH : core * 3 * CH + CH]
            mixed[rows, cols] = (gated * filtered).astype(BF16)

    def halo_copy(l):
        return rdma(halo.at[l, 0], halo.at[l, 1], sent.at[4], h_r.at[l], halo_next)

    def give_halo(l):
        halo[l, 0] = prod[ROWS:, :]
        start(halo_copy(l))

    def take_halo(l):
        with jax.named_scope("halo"):
            halo_copy(l).wait_recv()
        first = jnp.logical_and(s == 0, half == 0)
        prod[:8, :] = jnp.where(first, 0.0, halo[l, 1])

    def rs_copy(l, i, way, k, unit):
        lo, size = REDUCE[l][unit]
        rows = pl.ds(lo, size)
        return rdma(
            rs_out.at[l, way, k - 1, rows, :], rs_in.at[l, way, k - 1, rows, :],
            sent.at[3], ring_r.at[i * UNITS + unit], at_z(1 - 2 * way),
        )

    def partial(l, unit, chunk):
        lo, size = REDUCE[l][unit]
        return jnp.dot(mixed[lo : lo + size, :], w_out[:, aligned(chunk, PIECE)], preferred_element_type=F32)

    def rs_wait(l, i, unit):
        _, size = REDUCE[l][unit]
        ref = rs_in.at[l, 0, 0, pl.ds(0, size if i == 3 else 2 * size), :]
        rdma(ref, ref, sent.at[3], ring_r.at[i * UNITS + unit], partner).wait_recv()

    def arrived(l, way, k, unit):
        lo, size = REDUCE[l][unit]
        return rs_in[l, way, k - 1, lo : lo + size, :].astype(F32)

    def rs_step(l, i, unit):
        with jax.named_scope(f"rs#l={l}#i={i}#u={unit}"):
            lo, size = REDUCE[l][unit]
            moves = [(way, 4 - i if has(way, True, unit) else 3 - i) for way in range(2)]
            moves = [(way, k) for way, k in moves if k > 0]
            values = [partial(l, unit, chunk_at(k * (1 - 2 * way))) for way, k in moves]
            if i > 0:
                rs_wait(l, i - 1, unit)
            for (way, k), value in zip(moves, values):
                if i > 0:
                    value = value + arrived(l, way, k + 1, unit)
                rs_out[l, way, k - 1, lo : lo + size, :] = value.astype(BF16)
                start(rs_copy(l, i, way, k, unit))

    def rs_last(l, unit):
        with jax.named_scope(f"last#l={l}#u={unit}"):
            lo, size = REDUCE[l][unit]
            value = partial(l, unit, z)
            rs_wait(l, 3, unit)
            for way in range(2):
                value = value + arrived(l, way, 1, unit)
            return (x_all[l, z, lo : lo + size, :].astype(F32) + value).astype(BF16)

    def take_step(l, group, dist):
        for k in arrived_at(dist):
            take(l, group, chunk_at(k))
            if l == 1:
                multiply(l, group, chunk_at(k))

    ag_first(0, 0)
    ag_first(0, 1)
    w_stage(0, 0)
    w_stage(1, 0)
    start(rdma(res_other, x_all.at[0, z, :, own_cols], sent.at[4], m_r.at[0], partner))
    start(rdma(tap_all.at[c], tap_all.at[c], sent.at[5], m_r.at[1], partner))
    for unit in (3, 4, 2):
        ag_first(0, unit)
    start_sums()
    rdma(res_other, x_all.at[0, z, :, other_cols], sent.at[4], m_r.at[0], partner).wait_recv()
    take(0, 0, z)
    take(0, 1, z)

    w_stage(2, 0)
    w_stage(0, 1)
    ag_step(0, 0, 0)
    w_stage(1, 1)
    ag_step(0, 0, 1)
    take_step(0, 0, 0)
    ag_step(0, 0, 3)
    ag_step(0, 0, 4)
    w_stage(0, 2)
    ag_step(0, 0, 2)
    take_step(0, 1, 0)
    w_stage(2, 1)
    ag_step(0, 1, 0)
    w_stage(1, 2)
    w_stage(0, 3)
    ag_step(0, 1, 1)
    take_step(0, 0, 1)
    ag_step(0, 1, 3)
    ag_step(0, 1, 4)
    w_stage(1, 3)
    ag_step(0, 1, 2)
    take_step(0, 1, 1)
    w_stage(0, 4)
    ag_step(0, 2, 0)
    ag_step(0, 2, 1)
    take_step(0, 0, 2)
    w_stage(2, 2)
    w_stage(1, 4)
    ag_step(0, 2, 3)
    ag_step(0, 2, 4)
    w_end(0, 0)
    w_stage(2, 3)
    ag_step(0, 2, 2)
    take_step(0, 1, 2)
    w_end(0, -1, 1)
    ag_step(0, 3, 0)
    w_stage(2, 4)
    w_end(1, 0)
    ag_step(0, 3, 1)
    take_step(0, 0, 3)
    w_end(0, 2)
    w_taken(0, 0)
    multiply_row(0, 0, 0)
    for unit in (3, 4, 2):
        ag_step(0, 3, unit)
    take_step(0, 1, 3)
    w_end(1, -1, 1)
    w_taken(0, -1)
    multiply_row(0, 0, -1)
    w_taken(1, 0)
    build_w_out(0, 0)
    w_end(1, 2)
    w_stage(3, 0)
    w_taken(0, 1)
    multiply_row(0, 0, 1)
    for k in (-1, 1):
        w_taken(1, k)
        build_w_out(0, k)
    w_taken(0, 2)
    multiply_row(0, 0, 2)
    gates(0, 0)
    rdma(tap_all.at[other], tap_all.at[other], sent.at[4], m_r.at[1], partner).wait_recv()
    give_halo(0)
    mix(0, 0)
    mix(0, 1)
    w_taken(1, 2)
    build_w_out(0, 2)

    rs_step(0, 0, 0)
    rs_step(0, 0, 1)
    for k in (0, -1, 1, 2):
        multiply_row(0, 1, k)
    gates(0, 1)
    for unit in (3, 4):
        mix(0, unit)
        rs_step(0, 0, unit)
    rs_step(0, 1, 0)
    take_halo(0)
    mix(0, 2)
    rs_step(0, 0, 2)
    start_sums()
    for unit in (1, 3, 4):
        rs_step(0, 1, unit)
    w_stage(3, 1)
    rs_step(0, 2, 0)
    rs_step(0, 1, 2)
    for unit in (1, 3, 4):
        rs_step(0, 2, unit)
    rs_step(0, 3, 0)
    rs_step(0, 2, 2)
    w_stage(3, 2)
    for unit in (1, 3, 4):
        rs_step(0, 3, unit)

    def next_stream(unit):
        lo, size = REDUCE[0][unit]
        x_all[1, z, lo : lo + size, :] = rs_last(0, unit)
        ag_first(1, unit)

    next_stream(0)
    rs_step(0, 3, 2)
    w_stage(3, 3)
    next_stream(1)
    take(1, 0, z)
    next_stream(3)
    next_stream(4)

    ag_step(1, 0, 0)
    w_stage(3, 4)
    next_stream(2)
    take(1, 1, z)
    ag_step(1, 0, 1)
    ag_step(1, 0, 3)
    w_end(2, 0)
    w_end(2, -1, 1)
    ag_step(1, 0, 4)
    ag_step(1, 0, 2)
    ag_step(1, 1, 0)
    ag_step(1, 1, 1)
    w_end(2, 2)
    for unit in (3, 4, 2):
        ag_step(1, 1, unit)
    for k in (0, -1, 1, 2):
        w_taken(2, k)
        build_w_out(1, k)
    ag_step(1, 2, 0)
    for group in range(2):
        multiply(1, group, z)
        take_step(1, group, 0)
    ag_step(1, 2, 1)
    take_step(1, 0, 1)
    ag_step(1, 2, 3)
    take_step(1, 1, 1)
    ag_step(1, 2, 4)
    ag_step(1, 2, 2)
    take_step(1, 0, 2)
    take_step(1, 1, 2)
    for unit in (0, 1):
        ag_step(1, 3, unit)
        take_rows(1, GATHER[1][unit], chunk_at(4))
        multiply_rows(1, GATHER[1][unit], chunk_at(4))
        gates_rows(1, GATHER[1][unit])
        if unit == 1:
            give_halo(1)
        mix(1, unit)
        rs_step(1, 0, unit)
    for unit in (3, 4, 2):
        ag_step(1, 3, unit)
    take_step(1, 1, 3)
    gates(1, 1)
    for unit in (3, 4):
        mix(1, unit)
        rs_step(1, 0, unit)
    rs_step(1, 1, 0)
    take_halo(1)
    mix(1, 2)
    rs_step(1, 0, 2)
    for unit in (1, 3, 4):
        rs_step(1, 1, unit)
    rs_step(1, 2, 0)
    rs_step(1, 1, 2)
    for unit in (1, 3, 4):
        rs_step(1, 2, unit)
    rs_step(1, 3, 0)
    rs_step(1, 2, 2)
    for unit in (1, 3, 4, 2):
        rs_step(1, 3, unit)

    def fin_copy(group):
        rows = pl.ds(*span(REDUCE[1], group))
        return rdma(fin_out.at[rows, :], fin_in.at[rows, :], sent.at[4], m_r.at[2 + group], partner)

    def sums_copy(group, k, crossing):
        ref = sums.at[c, z, :, pl.ds(*span(REDUCE[1], group))]
        return rdma(ref, ref, sent.at[4], s_r.at[group, crossing], at_z(k, other if crossing else c))

    routes = [(4, 0), (4, 1), (3, 0), (3, 1), (5, 0), (5, 1), (2, 0), (2, 1), (6, 0), (6, 1)]
    routes += [(1, 0), (1, 1), (7, 0), (7, 1), (0, 1)]
    for group in range(2):
        for unit in ((0, 1), (3, 4, 2))[group]:
            lo, size = REDUCE[1][unit]
            st[lo : lo + size, :] = rs_last(1, unit).astype(F32)
        lo, size = span(REDUCE[1], group)
        rows = pl.ds(lo, size)
        value = st[rows, :]
        square = jnp.sum(value * value, axis=1, keepdims=True)
        sums[c, z, :, lo : lo + size] = jnp.broadcast_to(square, (size, 128)).T[:8, :]
        for k, crossing in routes:
            start(sums_copy(group, k, crossing))
        fin_out[rows, :] = st[rows, other_cols].astype(BF16)
        start(fin_copy(group))

    def scale_of(core):
        total = jnp.sum(sums[core, :, 0, :], axis=0, keepdims=True)
        return lax.rsqrt(jnp.broadcast_to(total, (128, ROWS)).T[:, :1] / D + FLOOR)

    with jax.named_scope("sums"):
        for group in range(2):
            fin_copy(group).wait_recv()
            cols = pl.ds(*span(REDUCE[1], group))
            for crossing, ref in enumerate((sums.at[c, pl.ds(0, NZ - 1), :, cols], sums.at[other, :, :, cols])):
                rdma(ref, ref, sent.at[4], s_r.at[group, crossing], partner).wait_recv()
    out[own_rows, :] = st[:, own_cols] * scale_of(c) * gain_out[...]
    out[other_rows, :] = fin_in[...].astype(F32) * scale_of(other) * gain_out[...]
    with jax.named_scope("sends"):
        for kind, rows in enumerate(SENT_ROWS):
            ref = w_all.at[0, pl.ds(0, rows), pl.ds(0, WIDE)] if rows <= D else w_all.at[0, pl.ds(0, rows // 2), :]
            rdma(ref, ref, sent.at[kind], m_r.at[0], partner).wait_send()
        rdma(tap_all.at[c], tap_all.at[c], sent.at[5], m_r.at[1], partner).wait_send()


def per_device(residual_in, norm_gain, gate_proj, filter_proj, signal_proj, conv_taps, out_proj, final_gain):
    dma = pltpu.SemaphoreType.DMA
    return pl.pallas_call(
        kernel,
        out_shape=jax.ShapeDtypeStruct((2 * ROWS, COLS), F32),
        in_specs=[pl.BlockSpec(memory_space=pltpu.HBM)] * 8,
        out_specs=pl.BlockSpec(memory_space=pltpu.VMEM),
        scratch_shapes=[
            pltpu.VMEM((LAYERS, NZ, ROWS, PIECE), BF16),
            pltpu.VMEM((ROWS, COLS), BF16),
            pltpu.VMEM((NZ, ROWS, PIECE), BF16),
            pltpu.VMEM((LAYERS, D, 2 * WIDE), BF16),
            pltpu.VMEM((2 * CH, D), BF16),
            pltpu.VMEM((ROWS, 6 * CH), F32),
            pltpu.VMEM((8 + ROWS, 2 * CH), F32),
            pltpu.VMEM((ROWS, 2 * CH), BF16),
            pltpu.VMEM((ROWS, 128), F32),
            pltpu.VMEM((LAYERS, 2, 4, ROWS, PIECE), BF16),
            pltpu.VMEM((LAYERS, 2, 4, ROWS, PIECE), BF16),
            pltpu.VMEM((LAYERS, 2, 8, 2 * CH), F32),
            pltpu.VMEM((2, TAPS, LAYERS, CH), F32),
            pltpu.VMEM((LAYERS, D), F32),
            pltpu.VMEM((1, COLS), F32),
            pltpu.VMEM((2, NZ, 8, ROWS), F32),
            pltpu.VMEM((ROWS, PIECE), F32),
            pltpu.VMEM((ROWS, COLS), BF16),
            pltpu.VMEM((ROWS, COLS), BF16),
            dma((1,)),
            dma((6,)),
            dma((4 * UNITS,)),
            dma((3, 20)),
            dma((3, SIDE)),
            dma((LAYERS,)),
            dma((2, 2)),
            dma((4,)),
        ],
        compiler_params=pltpu.CompilerParams(
            collective_id=0, has_side_effects=True, vmem_limit_bytes=44 * 1024 * 1024
        ),
    )(
        *(
            pltpu.with_memory_space_constraint(a, pltpu.HBM)
            for a in (
                residual_in, norm_gain, gate_proj, filter_proj, signal_proj, jnp.transpose(conv_taps, (1, 0, 2)),
                out_proj, final_gain.reshape(1, -1),
            )
        )
    )


def solution(mesh):
    return jax.shard_map(
        per_device,
        mesh=mesh,
        in_specs=(
            P("sp", "tp"),
            P(),
            P(None, "sp", "tp"),
            P(None, "sp", "tp"),
            P(None, "sp", "tp"),
            P(None, None, "tp"),
            P(None, "tp", "sp"),
            P("tp"),
        ),
        out_specs=P("sp", "tp"),
        check_vma=False,
    )
```

```python
import jax
import jax.numpy as jnp
from jax import lax
from jax.experimental import pallas as pl
from jax.experimental.pallas import tpu as pltpu
from jax.sharding import PartitionSpec as P

D = 4096
TAPS = 3
LAYERS = 2
FLOOR = 1e-06

NZ = 8
SIDE = 4
ROWS = 256
PIECE = 512
COLS = 256
CH = 128
WIDE = 512

F32 = jnp.float32
BF16 = jnp.bfloat16
MESH = pl.DeviceIdType.MESH

GATHER = (
    ((96, 80), (176, 80), (0, 16), (16, 48), (64, 32)),
    ((112, 80), (192, 64), (0, 16), (16, 48), (64, 48)),
)
REDUCE = (
    ((112, 80), (192, 64), (0, 16), (16, 48), (64, 48)),
    ((128, 64), (192, 64), (0, 16), (16, 64), (80, 48)),
)
GROUPS = ((0, 1), (2, 3, 4))
UNITS = 5
FAR = (0, 1, 1, 0, 1)

SENT_ROWS = (7680, 8192, 3584, 3584, 392)


def span(units, group):
    lo = units[GROUPS[group][0]][0]
    return lo, sum(units[u][1] for u in GROUPS[group])


def aligned(index, size):
    return pl.ds(pl.multiple_of(index * size, size), size)


def has(way, far, unit):
    return not far or FAR[unit] == way


def kernel(
    res, norm_gain, gate, filt, sig, taps, outp, final_gain, out,
    x_all, res_other, xg, w_all, w_out, acc, prod, mixed, sq, rs_out, rs_in, halo, tap_all, gain_in, gain_out,
    sums, st, fin_out, fin_in,
    loc, sent, ring_r, w_r, d_r, h_r, s_r, m_r,
):
    s = lax.axis_index("sp")
    t = lax.axis_index("tp")
    z, c = t // 2, t % 2
    y, x = s // SIDE, s % SIDE
    other = 1 - c
    partner = (s, 2 * z + other)

    def at_z(k, core=None):
        return (s, ((z + k + NZ) % NZ) * 2 + (c if core is None else core))

    def at_x(k):
        return (y * SIDE + (x + k + SIDE) % SIDE, t)

    def at_y(k):
        return (((y + k + SIDE) % SIDE) * SIDE + x, t)

    half = 1 - c
    halo_next = ((s + half) % 16, 2 * z + other)

    def rdma(src, dst, send, recv, device):
        return pltpu.make_async_remote_copy(
            src_ref=src, dst_ref=dst, send_sem=send, recv_sem=recv, device_id=device, device_id_type=MESH
        )

    def start(copy):
        copy.start()

    barrier = pltpu.get_barrier_semaphore()
    peers = [at_z(1), at_z(-1), at_z(1, other), at_z(-1, other), at_x(1), at_x(-1), at_y(1), at_y(-1), partner]
    for peer in peers:
        pl.semaphore_signal(barrier, inc=1, device_id=peer, device_id_type=MESH)

    own_cols = aligned(c, COLS)
    other_cols = aligned(other, COLS)
    own_rows = aligned(half, ROWS)
    other_rows = aligned(1 - half, ROWS)

    local = []

    def place(src, dst):
        copy = pltpu.make_async_copy(src, dst, loc.at[0])
        copy.start()
        local.append(copy)

    place(res.at[own_rows, :], x_all.at[0, z, :, own_cols])
    place(res.at[other_rows, :], res_other)
    for l in range(LAYERS):
        for part, ref in enumerate((gate, filt, sig)):
            first = pl.multiple_of(c * 3 * CH + (part + 1) * CH, CH)
            place(ref.at[l], w_all.at[l, aligned(s, 256), pl.ds(first, CH)])
        for h in range(2):
            place(
                outp.at[l, :, pl.ds(h * CH, CH)],
                w_all.at[l, aligned(2 * s + h, CH), aligned(c * 7, CH)],
            )
    place(norm_gain, gain_in)
    place(taps, tap_all.at[c])
    place(final_gain, gain_out)

    with jax.named_scope("barrier"):
        pl.semaphore_wait(barrier, len(peers))
    with jax.named_scope("local"):
        for copy in local:
            copy.wait()

    def lanes(what, core):
        if what == "proj":
            return pl.ds(pl.multiple_of(core * 3 * CH + CH, CH), 3 * CH)
        if what == "out":
            return aligned(core * 7, CH)
        return aligned(core, WIDE)

    carriers = ((0, "proj", 0, 64), (0, "proj", 64, 64), (0, "out", 0, 128), (1, "both", 0, 128))

    def w_copy(carrier, group, half, axis, across, sign, fwd, sending):
        l, what, first, size = carriers[carrier]
        step = sign if fwd else 0
        along = -step if sending else -step - sign
        lo = half * 128 + first
        if fwd:
            size = size // 2
            lo += 0 if sign == 1 else size
        if axis == 0:
            yy, xx = y + across, x + along
        else:
            yy, xx = y + along, x + across
        index = ((yy + SIDE) % SIDE) * SIDE + (xx + SIDE) % SIDE
        ref = w_all.at[l, pl.ds(pl.multiple_of(index * 256 + lo, 32), size), lanes(what, c)]
        slot = group * 2 + (1 if fwd else 0)
        device = at_x(sign) if axis == 0 else at_y(sign)
        return rdma(ref, ref, sent.at[0], w_r.at[carrier % 3, slot], device)

    groups = {("a", 1): (0, 0, 0, 0), ("b", 1): (5, 1, 1, 0)}
    for i, p in enumerate((0, -1, 1, 2)):
        groups["a", 2, p] = (1 + i, 0, 1, p)
        groups["b", 2, p] = (6 + i, 1, 0, p)

    def w_send(carrier, *name):
        group, half, axis, across = groups[name]
        for sign in (1, -1):
            start(w_copy(carrier, group, half, axis, across, sign, False, True))

    def w_wait(carrier, group, fwd):
        l, what, _, size = carriers[carrier]
        ref = w_all.at[l, pl.ds(0, size if fwd else 2 * size), lanes(what, c)]
        rdma(ref, ref, sent.at[0], w_r.at[carrier % 3, group * 2 + (1 if fwd else 0)], partner).wait_recv()

    def w_forward(carrier, *name):
        group, half, axis, across = groups[name]
        w_wait(carrier, group, False)
        for sign in (1, -1):
            start(w_copy(carrier, group, half, axis, across, sign, True, True))

    def w_finish(carrier, *name):
        w_wait(carrier, groups[name][0], True)

    parcels = ((0, "proj"), (0, "out"), (1, "both"))

    def w_parcel(parcel, k, core):
        l, what = parcels[parcel]
        ref = w_all.at[l, aligned((y + k + SIDE) % SIDE, 1024), lanes(what, core)]
        slot = (k + SIDE) % SIDE
        return rdma(ref, ref, sent.at[1], d_r.at[parcel, slot], partner)

    def w_hand(parcel, *ks):
        for k in ks:
            start(w_parcel(parcel, k, c))

    def w_taken(parcel, k):
        with jax.named_scope(f"taken#p={parcel}#k={k}"):
            w_parcel(parcel, k, other).wait_recv()

    def w_stage(carrier, stage):
        with jax.named_scope(f"w#t={carrier}#s={stage}"):
            w_stage_body(carrier, stage)

    def w_stage_body(t, stage):
        if stage == 0:
            w_send(t, "a", 1)
            w_send(t, "b", 1)
            w_send(t, "b", 2, 0)
            w_send(t, "a", 2, 0)
        elif stage == 1:
            w_forward(t, "a", 1)
            w_forward(t, "b", 1)
            for p in (-1, 1):
                w_send(t, "a", 2, p)
                w_send(t, "b", 2, p)
            w_forward(t, "b", 2, 0)
            w_forward(t, "a", 2, 0)
        elif stage == 2:
            w_finish(t, "a", 1)
            w_send(t, "a", 2, 2)
            w_finish(t, "b", 1)
            w_send(t, "b", 2, 2)
        elif stage == 3:
            for p in (-1, 1):
                w_forward(t, "a", 2, p)
                w_forward(t, "b", 2, p)
        else:
            w_forward(t, "a", 2, 2)
            w_forward(t, "b", 2, 2)

    def w_end(parcel, *ks):
        with jax.named_scope(f"end#p={parcel}#k={ks[0]}"):
            for k in ks:
                for t in ((0, 1), (2,), (3,))[parcel]:
                    w_finish(t, "a", 2, k)
                    w_finish(t, "b", 2, k)
        w_hand(parcel, *ks)

    def build_w_out(l, k):
        first = ((y + k + SIDE) % SIDE) * 8

        def body(i, carry):
            for core in range(2):
                w_out[core * CH : (core + 1) * CH, aligned(first + i, CH)] = w_all[
                    l, aligned(first + i, CH), core * 7 * CH : (core * 7 + 1) * CH
                ]
            return carry

        lax.fori_loop(0, 8, body, 0)

    def chunk_at(k):
        return (z + k + NZ) % NZ

    def ag_copy(l, way, dist, unit):
        sign = 1 - 2 * way
        lo, size = GATHER[l][unit]
        ref = x_all.at[l, chunk_at(-sign * dist), pl.ds(lo, size), :]
        return rdma(ref, ref, sent.at[2], ring_r.at[dist * UNITS + unit], at_z(sign))

    def first_copy(way, unit, crossing):
        lo, size = GATHER[0][unit]
        dst = x_all.at[0, z, pl.ds(lo, size), own_cols]
        src = res_other.at[pl.ds(lo, size), :] if crossing else dst
        return rdma(src, dst, sent.at[2], ring_r.at[unit], at_z(1 - 2 * way, other if crossing else c))

    def ag_first(l, unit):
        for way in range(2):
            if l == 0:
                start(first_copy(way, unit, False))
                start(first_copy(way, unit, True))
            else:
                start(ag_copy(l, way, 0, unit))

    def ag_step(l, dist, unit):
        with jax.named_scope(f"ag#l={l}#d={dist}#u={unit}"):
            _, size = GATHER[l][unit]
            ref = x_all.at[l, 0, pl.ds(0, size if dist == 3 else 2 * size), :]
            rdma(ref, ref, sent.at[2], ring_r.at[dist * UNITS + unit], partner).wait_recv()
            for way in range(2):
                if dist < 3 and has(way, dist == 2, unit):
                    start(ag_copy(l, way, dist + 1, unit))

    def take(l, group, chunk):
        take_rows(l, span(GATHER[l], group), chunk)

    def take_rows(l, which, chunk):
        lo, size = which
        rows = pl.ds(lo, size)
        value = x_all[l, chunk, rows, :].astype(F32)
        square = value * value
        total = square[:, :128]
        for i in range(1, PIECE // 128):
            total = total + square[:, i * 128 : (i + 1) * 128]
        sq[rows, :] += total
        xg[chunk, rows, :] = (value * gain_in[l : l + 1, aligned(chunk, PIECE)]).astype(BF16)

    def arrived_at(dist):
        return (-dist - 1, dist + 1) if dist < 3 else (4,)

    def multiply(l, group, chunk):
        multiply_rows(l, span(GATHER[l], group), chunk)

    def multiply_rows(l, which, chunk):
        lo, size = which
        acc[lo : lo + size, :] += jnp.dot(
            xg[chunk, lo : lo + size, :],
            w_all[l, aligned(chunk, PIECE), CH : 7 * CH],
            preferred_element_type=F32,
        )

    def multiply_row(l, group, k):
        first = ((y + k + SIDE) % SIDE) * 2
        with jax.named_scope(f"mult#g={group}"):
            multiply(l, group, first)
            multiply(l, group, first + 1)

    def start_sums():
        sq[...] = jnp.zeros_like(sq)
        acc[...] = jnp.zeros_like(acc)

    def gates(l, group):
        gates_rows(l, span(GATHER[l], group))

    def gates_rows(l, which):
        lo, size = which
        rows = pl.ds(lo, size)
        mean = jnp.sum(sq[rows, :], axis=1, keepdims=True) / D
        scale = lax.rsqrt(mean + FLOOR)
        for core in range(2):
            base = core * 3 * CH
            value = (acc[rows, base + CH : base + 2 * CH] * scale) * (acc[rows, base + 2 * CH : base + 3 * CH] * scale)
            prod[pl.ds(8 + lo, size), core * CH : (core + 1) * CH] = value.astype(BF16).astype(F32)
            acc[rows, base : base + CH] = acc[rows, base : base + CH] * scale

    def mix(l, unit):
        lo, size = REDUCE[l][unit]
        rows = pl.ds(lo, size)
        for core in range(2):
            cols = pl.ds(core * CH, CH)
            filtered = jnp.zeros((size, CH), F32)
            for k in range(TAPS):
                tap = tap_all[core, k, l : l + 1, :]
                filtered = filtered + tap * prod[pl.ds(8 + lo - (TAPS - 1) + k, size), cols]
            gated = acc[rows, core * 3 * CH : core * 3 * CH + CH]
            mixed[rows, cols] = (gated * filtered).astype(BF16)

    def halo_copy(l):
        return rdma(halo.at[l, 0], halo.at[l, 1], sent.at[4], h_r.at[l], halo_next)

    def give_halo(l):
        halo[l, 0] = prod[ROWS:, :]
        start(halo_copy(l))

    def take_halo(l):
        with jax.named_scope("halo"):
            halo_copy(l).wait_recv()
        first = jnp.logical_and(s == 0, half == 0)
        prod[:8, :] = jnp.where(first, 0.0, halo[l, 1])

    def rs_copy(l, i, way, k, unit):
        lo, size = REDUCE[l][unit]
        rows = pl.ds(lo, size)
        return rdma(
            rs_out.at[l, way, k - 1, rows, :], rs_in.at[l, way, k - 1, rows, :],
            sent.at[3], ring_r.at[i * UNITS + unit], at_z(1 - 2 * way),
        )

    def partial(l, unit, chunk):
        lo, size = REDUCE[l][unit]
        return jnp.dot(mixed[lo : lo + size, :], w_out[:, aligned(chunk, PIECE)], preferred_element_type=F32)

    def rs_wait(l, i, unit):
        _, size = REDUCE[l][unit]
        ref = rs_in.at[l, 0, 0, pl.ds(0, size if i == 3 else 2 * size), :]
        rdma(ref, ref, sent.at[3], ring_r.at[i * UNITS + unit], partner).wait_recv()

    def arrived(l, way, k, unit):
        lo, size = REDUCE[l][unit]
        return rs_in[l, way, k - 1, lo : lo + size, :].astype(F32)

    def rs_step(l, i, unit):
        with jax.named_scope(f"rs#l={l}#i={i}#u={unit}"):
            lo, size = REDUCE[l][unit]
            moves = [(way, 4 - i if has(way, True, unit) else 3 - i) for way in range(2)]
            moves = [(way, k) for way, k in moves if k > 0]
            values = [partial(l, unit, chunk_at(k * (1 - 2 * way))) for way, k in moves]
            if i > 0:
                rs_wait(l, i - 1, unit)
            for (way, k), value in zip(moves, values):
                if i > 0:
                    value = value + arrived(l, way, k + 1, unit)
                rs_out[l, way, k - 1, lo : lo + size, :] = value.astype(BF16)
                start(rs_copy(l, i, way, k, unit))

    def rs_last(l, unit):
        with jax.named_scope(f"last#l={l}#u={unit}"):
            lo, size = REDUCE[l][unit]
            value = partial(l, unit, z)
            rs_wait(l, 3, unit)
            for way in range(2):
                value = value + arrived(l, way, 1, unit)
            return (x_all[l, z, lo : lo + size, :].astype(F32) + value).astype(BF16)

    def take_step(l, group, dist):
        for k in arrived_at(dist):
            take(l, group, chunk_at(k))
            if l == 1:
                multiply(l, group, chunk_at(k))

    ag_first(0, 0)
    ag_first(0, 1)
    w_stage(0, 0)
    w_stage(1, 0)
    start(rdma(res_other, x_all.at[0, z, :, own_cols], sent.at[4], m_r.at[0], partner))
    start(rdma(tap_all.at[c], tap_all.at[c], sent.at[5], m_r.at[1], partner))
    for unit in (3, 4, 2):
        ag_first(0, unit)
    start_sums()
    rdma(res_other, x_all.at[0, z, :, other_cols], sent.at[4], m_r.at[0], partner).wait_recv()
    take(0, 0, z)
    take(0, 1, z)

    w_stage(2, 0)
    w_stage(0, 1)
    ag_step(0, 0, 0)
    w_stage(1, 1)
    ag_step(0, 0, 1)
    take_step(0, 0, 0)
    ag_step(0, 0, 3)
    ag_step(0, 0, 4)
    w_stage(0, 2)
    ag_step(0, 0, 2)
    take_step(0, 1, 0)
    w_stage(2, 1)
    ag_step(0, 1, 0)
    w_stage(1, 2)
    w_stage(0, 3)
    ag_step(0, 1, 1)
    take_step(0, 0, 1)
    ag_step(0, 1, 3)
    ag_step(0, 1, 4)
    w_stage(1, 3)
    ag_step(0, 1, 2)
    take_step(0, 1, 1)
    w_stage(0, 4)
    ag_step(0, 2, 0)
    ag_step(0, 2, 1)
    take_step(0, 0, 2)
    w_stage(2, 2)
    w_stage(1, 4)
    ag_step(0, 2, 3)
    ag_step(0, 2, 4)
    w_end(0, 0)
    w_stage(2, 3)
    ag_step(0, 2, 2)
    take_step(0, 1, 2)
    w_end(0, -1, 1)
    ag_step(0, 3, 0)
    w_stage(2, 4)
    w_end(1, 0)
    ag_step(0, 3, 1)
    take_step(0, 0, 3)
    w_end(0, 2)
    w_taken(0, 0)
    multiply_row(0, 0, 0)
    for unit in (3, 4, 2):
        ag_step(0, 3, unit)
    take_step(0, 1, 3)
    w_end(1, -1, 1)
    w_taken(0, -1)
    multiply_row(0, 0, -1)
    w_taken(1, 0)
    build_w_out(0, 0)
    w_end(1, 2)
    w_stage(3, 0)
    w_taken(0, 1)
    multiply_row(0, 0, 1)
    for k in (-1, 1):
        w_taken(1, k)
        build_w_out(0, k)
    w_taken(0, 2)
    multiply_row(0, 0, 2)
    gates(0, 0)
    rdma(tap_all.at[other], tap_all.at[other], sent.at[4], m_r.at[1], partner).wait_recv()
    give_halo(0)
    mix(0, 0)
    mix(0, 1)
    w_taken(1, 2)
    build_w_out(0, 2)

    rs_step(0, 0, 0)
    rs_step(0, 0, 1)
    for k in (0, -1, 1, 2):
        multiply_row(0, 1, k)
    gates(0, 1)
    for unit in (3, 4):
        mix(0, unit)
        rs_step(0, 0, unit)
    rs_step(0, 1, 0)
    take_halo(0)
    mix(0, 2)
    rs_step(0, 0, 2)
    start_sums()
    for unit in (1, 3, 4):
        rs_step(0, 1, unit)
    w_stage(3, 1)
    rs_step(0, 2, 0)
    rs_step(0, 1, 2)
    for unit in (1, 3, 4):
        rs_step(0, 2, unit)
    rs_step(0, 3, 0)
    rs_step(0, 2, 2)
    w_stage(3, 2)
    for unit in (1, 3, 4):
        rs_step(0, 3, unit)

    def next_stream(unit):
        lo, size = REDUCE[0][unit]
        x_all[1, z, lo : lo + size, :] = rs_last(0, unit)
        ag_first(1, unit)

    next_stream(0)
    rs_step(0, 3, 2)
    w_stage(3, 3)
    next_stream(1)
    take(1, 0, z)
    next_stream(3)
    next_stream(4)

    ag_step(1, 0, 0)
    w_stage(3, 4)
    next_stream(2)
    take(1, 1, z)
    ag_step(1, 0, 1)
    ag_step(1, 0, 3)
    w_end(2, 0)
    w_end(2, -1, 1)
    ag_step(1, 0, 4)
    ag_step(1, 0, 2)
    ag_step(1, 1, 0)
    ag_step(1, 1, 1)
    w_end(2, 2)
    for unit in (3, 4, 2):
        ag_step(1, 1, unit)
    for k in (0, -1, 1, 2):
        w_taken(2, k)
        build_w_out(1, k)
    ag_step(1, 2, 0)
    for group in range(2):
        multiply(1, group, z)
        take_step(1, group, 0)
    ag_step(1, 2, 1)
    take_step(1, 0, 1)
    ag_step(1, 2, 3)
    take_step(1, 1, 1)
    ag_step(1, 2, 4)
    ag_step(1, 2, 2)
    take_step(1, 0, 2)
    take_step(1, 1, 2)
    for unit in (0, 1):
        ag_step(1, 3, unit)
        take_rows(1, GATHER[1][unit], chunk_at(4))
        multiply_rows(1, GATHER[1][unit], chunk_at(4))
        gates_rows(1, GATHER[1][unit])
        if unit == 1:
            give_halo(1)
        mix(1, unit)
        rs_step(1, 0, unit)
    for unit in (3, 4, 2):
        ag_step(1, 3, unit)
    take_step(1, 1, 3)
    gates(1, 1)
    for unit in (3, 4):
        mix(1, unit)
        rs_step(1, 0, unit)
    rs_step(1, 1, 0)
    take_halo(1)
    mix(1, 2)
    rs_step(1, 0, 2)
    for unit in (1, 3, 4):
        rs_step(1, 1, unit)
    rs_step(1, 2, 0)
    rs_step(1, 1, 2)
    for unit in (1, 3, 4):
        rs_step(1, 2, unit)
    rs_step(1, 3, 0)
    rs_step(1, 2, 2)
    for unit in (1, 3, 4, 2):
        rs_step(1, 3, unit)

    def fin_copy(group):
        rows = pl.ds(*span(REDUCE[1], group))
        return rdma(fin_out.at[rows, :], fin_in.at[rows, :], sent.at[4], m_r.at[2 + group], partner)

    def sums_copy(group, k, crossing):
        ref = sums.at[c, z, :, pl.ds(*span(REDUCE[1], group))]
        return rdma(ref, ref, sent.at[4], s_r.at[group, crossing], at_z(k, other if crossing else c))

    routes = [(4, 0), (4, 1), (3, 0), (3, 1), (5, 0), (5, 1), (2, 0), (2, 1), (6, 0), (6, 1)]
    routes += [(1, 0), (1, 1), (7, 0), (7, 1), (0, 1)]
    for group in range(2):
        for unit in ((0, 1), (3, 4, 2))[group]:
            lo, size = REDUCE[1][unit]
            st[lo : lo + size, :] = rs_last(1, unit).astype(F32)
        lo, size = span(REDUCE[1], group)
        rows = pl.ds(lo, size)
        value = st[rows, :]
        square = jnp.sum(value * value, axis=1, keepdims=True)
        sums[c, z, :, lo : lo + size] = jnp.broadcast_to(square, (size, 128)).T[:8, :]
        for k, crossing in routes:
            start(sums_copy(group, k, crossing))
        fin_out[rows, :] = st[rows, other_cols].astype(BF16)
        start(fin_copy(group))

    def scale_of(core):
        total = jnp.sum(sums[core, :, 0, :], axis=0, keepdims=True)
        return lax.rsqrt(jnp.broadcast_to(total, (128, ROWS)).T[:, :1] / D + FLOOR)

    out[own_rows, :] = st[:, own_cols] * gain_out[...]
    with jax.named_scope("sums"):
        for group in range(2):
            fin_copy(group).wait_recv()
        out[other_rows, :] = fin_in[...].astype(F32) * gain_out[...]
        for group in range(2):
            cols = pl.ds(*span(REDUCE[1], group))
            for crossing, ref in enumerate((sums.at[c, pl.ds(0, NZ - 1), :, cols], sums.at[other, :, :, cols])):
                rdma(ref, ref, sent.at[4], s_r.at[group, crossing], partner).wait_recv()
    out[own_rows, :] = out[own_rows, :] * scale_of(c)
    out[other_rows, :] = out[other_rows, :] * scale_of(other)
    with jax.named_scope("sends"):
        for kind, rows in enumerate(SENT_ROWS):
            ref = w_all.at[0, pl.ds(0, rows), pl.ds(0, WIDE)] if rows <= D else w_all.at[0, pl.ds(0, rows // 2), :]
            rdma(ref, ref, sent.at[kind], m_r.at[0], partner).wait_send()
        rdma(tap_all.at[c], tap_all.at[c], sent.at[5], m_r.at[1], partner).wait_send()


def per_device(residual_in, norm_gain, gate_proj, filter_proj, signal_proj, conv_taps, out_proj, final_gain):
    dma = pltpu.SemaphoreType.DMA
    return pl.pallas_call(
        kernel,
        out_shape=jax.ShapeDtypeStruct((2 * ROWS, COLS), F32),
        in_specs=[pl.BlockSpec(memory_space=pltpu.HBM)] * 8,
        out_specs=pl.BlockSpec(memory_space=pltpu.VMEM),
        scratch_shapes=[
            pltpu.VMEM((LAYERS, NZ, ROWS, PIECE), BF16),
            pltpu.VMEM((ROWS, COLS), BF16),
            pltpu.VMEM((NZ, ROWS, PIECE), BF16),
            pltpu.VMEM((LAYERS, D, 2 * WIDE), BF16),
            pltpu.VMEM((2 * CH, D), BF16),
            pltpu.VMEM((ROWS, 6 * CH), F32),
            pltpu.VMEM((8 + ROWS, 2 * CH), F32),
            pltpu.VMEM((ROWS, 2 * CH), BF16),
            pltpu.VMEM((ROWS, 128), F32),
            pltpu.VMEM((LAYERS, 2, 4, ROWS, PIECE), BF16),
            pltpu.VMEM((LAYERS, 2, 4, ROWS, PIECE), BF16),
            pltpu.VMEM((LAYERS, 2, 8, 2 * CH), F32),
            pltpu.VMEM((2, TAPS, LAYERS, CH), F32),
            pltpu.VMEM((LAYERS, D), F32),
            pltpu.VMEM((1, COLS), F32),
            pltpu.VMEM((2, NZ, 8, ROWS), F32),
            pltpu.VMEM((ROWS, PIECE), F32),
            pltpu.VMEM((ROWS, COLS), BF16),
            pltpu.VMEM((ROWS, COLS), BF16),
            dma((1,)),
            dma((6,)),
            dma((4 * UNITS,)),
            dma((3, 20)),
            dma((3, SIDE)),
            dma((LAYERS,)),
            dma((2, 2)),
            dma((4,)),
        ],
        compiler_params=pltpu.CompilerParams(
            collective_id=0, has_side_effects=True, vmem_limit_bytes=44 * 1024 * 1024
        ),
    )(
        *(
            pltpu.with_memory_space_constraint(a, pltpu.HBM)
            for a in (
                residual_in, norm_gain, gate_proj, filter_proj, signal_proj, jnp.transpose(conv_taps, (1, 0, 2)),
                out_proj, final_gain.reshape(1, -1),
            )
        )
    )


def solution(mesh):
    return jax.shard_map(
        per_device,
        mesh=mesh,
        in_specs=(
            P("sp", "tp"),
            P(),
            P(None, "sp", "tp"),
            P(None, "sp", "tp"),
            P(None, "sp", "tp"),
            P(None, None, "tp"),
            P(None, "tp", "sp"),
            P("tp"),
        ),
        out_specs=P("sp", "tp"),
        check_vma=False,
    )
```
